32 devices in a mesh: kv: 8 (over z, y), tp: 4 (over x, core).
Axes of the slice: x: 2, y: 2, z: 4, core: 2. Of those that a mesh axis runs over, the one named last changes fastest.
Arguments:
- tokens: bfloat16 [1024, 4096], P(None, 'kv'), may hold values from -6 to 6
- norm_gain: float32 [4096], replicated, may hold values from 0.1 to 1.9
- query_weight: bfloat16 [4096, 2048], P('kv', 'tp'), may hold values from -0.09375 to 0.09375
- key_weight: bfloat16 [4096, 2048], P('kv', 'tp'), may hold values from -0.09375 to 0.09375
- value_weight: bfloat16 [4096, 4096], P('kv', 'tp'), may hold values from -0.09375 to 0.09375
- outgate_weight: bfloat16 [4096, 4096], P('kv', 'tp'), may hold values from -0.09375 to 0.09375
- gate_weight: bfloat16 [4096, 32], P('kv'), may hold values from -0.09375 to 0.09375
- forget_bias: float32 [16], replicated, may hold values from -1 to 5
- head_gain: float32 [4096], P('tp'), may hold values from 0.1 to 1.9
- output_weight: bfloat16 [4096, 4096], P('tp', 'kv'), may hold values from -0.09375 to 0.09375
- state_matrix: float32 [256, 16, 128, 256], P('kv', 'tp'), may hold values from -6 to 6
- state_normal: float32 [256, 16, 128], P('kv', 'tp'), may hold values from -6 to 6
- state_stable: float32 [256, 16], P('kv', 'tp'), may hold values from -3 to 3
- prior_keys: bfloat16 [256, 4, 2048], P('kv', None, 'tp'), may hold values from -0.59765625 to 0.59765625
- prior_values: bfloat16 [256, 4, 4096], P('kv', None, 'tp'), may hold values from -6 to 6
- prior_ingate: float32 [256, 4, 16], P('kv', None, 'tp'), may hold values from -4 to 4
- prior_forget: float32 [256, 4, 16], P('kv', None, 'tp'), may hold values from -2 to -0.02
- accepted: int32 [256], P('kv'), may hold values from 0 to 4
- parents: int32 [256, 4], P('kv'), may hold values from -1 to 2, as said below
Outputs:
- layer_out: bfloat16 [1024, 4096], P('tp', 'kv')
- new_matrix: float32 [256, 16, 128, 256], P('kv', 'tp')
- new_normal: float32 [256, 16, 128], P('kv', 'tp')
- new_stable: float32 [256, 16], P('kv', 'tp')
The draws below stay inside these ranges and needn't reach their ends.
Inputs may be any that keep to these rules, and one draw needn't show every extreme that they name: parents of proposal t lie in -1 to t - 1; the first proposal's parent is -1; in some sequence each proposal's parent is the one before it.
All inputs are finite; a program needn't handle non-finite values.
Results may differ from the reference program's by a relative error of at most 0.0089.
Values may be sent and summed in bfloat16 or wider, within the bound.
A program may use at most 128 MiB of HBM per device.

```python
import jax
import jax.numpy as jnp
from jax import lax

D = 4096
HEADS = 16
DQK = 128
DV = 256
PROP = 4
SEQS = 256
TOKENS = 1024


def draw_parents(key, part):
    random_ints = jax.random.randint(key, (SEQS, PROP), 0, 1 << 20)
    position = jnp.arange(PROP, dtype=jnp.int32)[None, :]
    chosen = random_ints % jnp.maximum(position, 1)
    leading = jnp.arange(SEQS, dtype=jnp.int32)[:, None] == 0
    chosen = jnp.where(leading, position - 1, chosen)
    return jnp.where(position == 0, -1, chosen).astype(jnp.int32)


def set_ends(entries, rng, least, top_value):
    dims = entries.shape
    place = [jax.random.randint(jax.random.fold_in(rng, axis), (), 0, dims[axis]) for axis in range(len(dims))]
    entries = entries.at[tuple(place)].set(least)
    longest = dims.index(max(dims))
    place[longest] = (place[longest] + 1) % dims[longest]
    return entries.at[tuple(place)].set(top_value)


def block_scale(rng, shape, shards, least, largest):
    def one(axis_at, parts):
        steps = jax.random.uniform(jax.random.fold_in(jax.random.fold_in(rng, 6), axis_at), (parts,), jnp.float32, least / len(shards), largest / len(shards))
        return jnp.repeat(jnp.exp(steps), shape[axis_at] // parts).reshape((-1,) + (1,) * (len(shape) - axis_at - 1))

    factor_of = one(*shards[0])
    for cut in shards[1:]:
        factor_of = factor_of * one(*cut)
    return factor_of


def centred(rng, dims, scale, most, shards=(), kind=jnp.bfloat16):
    loudness = block_scale(rng, dims, shards, -0.22, 0.18) if shards else 1.0
    array = jax.random.normal(rng, dims, jnp.float32) * scale * loudness
    return jnp.minimum(jnp.maximum(array, -most), most).astype(kind)


def setup_inputs(seed: int = 0) -> dict:
    keys = jax.random.split(jax.random.key(seed), 20)
    return {
        "tokens": centred(keys[0], (TOKENS, D), 1.0, 6.0, ((1, 8),)),
        "norm_gain": jnp.clip(1.0 + 0.18 * jax.random.normal(keys[1], (D,), jnp.float32), 0.1, 1.9),
        "query_weight": centred(keys[2], (D, HEADS * DQK), D ** -0.5, 0.09375, ((0, 8), (1, 4))),
        "key_weight": centred(keys[3], (D, HEADS * DQK), D ** -0.5, 0.09375, ((0, 8), (1, 4))),
        "value_weight": centred(keys[4], (D, HEADS * DV), D ** -0.5, 0.09375, ((0, 8), (1, 4))),
        "outgate_weight": centred(keys[5], (D, HEADS * DV), D ** -0.5, 0.09375, ((0, 8), (1, 4))),
        "gate_weight": centred(keys[6], (D, 2 * HEADS), D ** -0.5, 0.09375, ((0, 8),)),
        "forget_bias": jnp.clip(jax.random.uniform(keys[7], (HEADS,), jnp.float32, -1.0, 5.0), -1.0, 5.0),
        "head_gain": jnp.clip(1.0 + 0.18 * jax.random.normal(keys[8], (HEADS * DV,), jnp.float32), 0.1, 1.9),
        "output_weight": centred(keys[9], (HEADS * DV, D), (HEADS * DV) ** -0.5, 0.09375, ((0, 4), (1, 8))),
        "state_matrix": centred(keys[10], (SEQS, HEADS, DQK, DV), 1.0, 6.0, ((0, 8), (1, 4)), jnp.float32),
        "state_normal": centred(keys[11], (SEQS, HEADS, DQK), 1.0, 6.0, ((0, 8), (1, 4)), jnp.float32),
        "state_stable": centred(keys[12], (SEQS, HEADS), 1.0, 3.0, ((0, 8), (1, 4)), jnp.float32),
        "prior_keys": centred(keys[13], (SEQS, PROP, HEADS * DQK), 0.09, 0.59765625, ((0, 8), (2, 4))),
        "prior_values": centred(keys[14], (SEQS, PROP, HEADS * DV), 1.0, 6.0, ((0, 8), (2, 4))),
        "prior_ingate": centred(keys[15], (SEQS, PROP, HEADS), 1.0, 4.0, ((0, 8), (2, 4)), jnp.float32),
        "prior_forget": jnp.clip(-2.0 + 1.98 * jax.random.uniform(keys[16], (SEQS, PROP, HEADS), jnp.float32) ** block_scale(keys[16], (SEQS, PROP, HEADS), ((0, 8), (2, 4)), -0.2, 0.2), -2.0, -0.02),
        "accepted": set_ends(jax.random.randint(keys[17], (SEQS,), 0, PROP + 1), jax.random.fold_in(keys[17], 1), 0, PROP).astype(jnp.int32),
        "parents": draw_parents(jax.random.fold_in(keys[19], 71), 0),
    }


def ancestry(parents):
    count = parents.shape[1]
    index = jnp.arange(count, dtype=jnp.int32)
    current = jnp.broadcast_to(index[None, :], parents.shape).astype(jnp.int32)
    table = jnp.broadcast_to((index[:, None] == index[None, :]).astype(jnp.float32), (parents.shape[0], count, count))
    for repeat in range(count - 1):
        looked = jnp.take_along_axis(parents, jnp.maximum(current, 0), axis=1)
        current = jnp.where(current >= 0, looked, -1).astype(jnp.int32)
        table = table + (current[:, :, None] == index[None, None, :]).astype(jnp.float32)
    return table

def commit(matrix, normal, stable, prior_k, prior_v, prior_i, prior_f, accepted):
    count = prior_k.shape[1]
    live = (jnp.arange(count, dtype=jnp.int32)[None, :] < accepted[:, None])[:, :, None]
    forget_live = jnp.where(live, prior_f, 0.0)
    cumul = jnp.cumsum(forget_live, axis=1)
    total = cumul[:, -1]
    weight_log = jnp.where(live, total[:, None, :] - cumul + prior_i, -jnp.inf)
    new_stable = jnp.maximum(total + stable, lax.optimization_barrier(jnp.max(weight_log, axis=1)))
    weights = jnp.exp(weight_log - new_stable[:, None, :])
    decay = jnp.exp(total + stable - new_stable)
    hp = lax.Precision.HIGHEST
    new_matrix = decay[:, :, None, None] * matrix + jnp.einsum('sph,sphd,sphv->shdv', weights, prior_k, prior_v, precision=hp)
    new_normal = decay[:, :, None] * normal + jnp.einsum('sph,sphd->shd', weights, prior_k, precision=hp)
    return (new_matrix, new_normal, new_stable)

def tree_read(query, key_rows, value_rows, ingate, logforget, table, matrix, normal, stable):
    hp = lax.Precision.HIGHEST
    path_sum = jnp.einsum('sta,sah->sth', table, logforget, precision=hp)
    dlog = path_sum[:, :, None, :] - path_sum[:, None, :, :] + ingate[:, None, :, :]
    dlog = jnp.where(table[:, :, :, None] > 0.5, dlog, -jnp.inf)
    carried = path_sum + stable[:, None, :]
    top = jnp.maximum(carried, lax.optimization_barrier(jnp.max(dlog, axis=2)))
    scores = jnp.einsum('sthd,sahd->stah', query, key_rows, precision=hp) * jnp.exp(dlog - top[:, :, None, :])
    factor = jnp.exp(carried - top)
    numer = jnp.einsum('stah,sahv->sthv', scores, value_rows, precision=hp) + factor[..., None] * jnp.einsum('sthd,shdv->sthv', query, matrix, precision=hp)
    denom = lax.optimization_barrier(jnp.sum(scores, axis=2)) + factor * jnp.einsum('sthd,shd->sth', query, normal, precision=hp)
    return numer / jnp.maximum(jnp.abs(denom), jnp.exp(-top))[..., None]

def reference(tokens, norm_gain, query_weight, key_weight, value_weight, outgate_weight, gate_weight, forget_bias, head_gain, output_weight, state_matrix, state_normal, state_stable, prior_keys, prior_values, prior_ingate, prior_forget, accepted, parents):
    f32 = jnp.float32
    xfloat = tokens.astype(f32)
    scale = lax.rsqrt(lax.optimization_barrier(jnp.sum(xfloat * xfloat, axis=-1, keepdims=True)) / D + 1e-06)
    normed = (xfloat * norm_gain).astype(jnp.bfloat16)
    query = scale * jnp.dot(normed, query_weight, preferred_element_type=f32)
    key_rows = scale * jnp.dot(normed, key_weight, preferred_element_type=f32) / jnp.sqrt(jnp.float32(DQK))
    value_rows = scale * jnp.dot(normed, value_weight, preferred_element_type=f32)
    outgate = scale * jnp.dot(normed, outgate_weight, preferred_element_type=f32)
    gates = scale * jnp.dot(normed, gate_weight, preferred_element_type=f32)
    ingate = gates[:, :HEADS].reshape(SEQS, PROP, HEADS)
    logforget = jax.nn.log_sigmoid(gates[:, HEADS:] + forget_bias).reshape(SEQS, PROP, HEADS)
    new_matrix, new_normal, new_stable = commit(state_matrix, state_normal, state_stable, prior_keys.astype(f32).reshape(SEQS, PROP, HEADS, DQK), prior_values.astype(f32).reshape(SEQS, PROP, HEADS, DV), prior_ingate, prior_forget, accepted)
    table = ancestry(parents)
    read = tree_read(query.reshape(SEQS, PROP, HEADS, DQK), key_rows.reshape(SEQS, PROP, HEADS, DQK), value_rows.reshape(SEQS, PROP, HEADS, DV), ingate, logforget, table, new_matrix, new_normal, new_stable)
    normer = lax.rsqrt(lax.optimization_barrier(jnp.mean(read * read, axis=-1, keepdims=True)) + 1e-06)
    hidden = read * normer * head_gain.reshape(HEADS, DV) * jax.nn.sigmoid(outgate.reshape(SEQS, PROP, HEADS, DV))
    hidden = hidden.reshape(TOKENS, HEADS * DV).astype(jnp.bfloat16)
    layer_out = jnp.dot(hidden, output_weight, preferred_element_type=f32).astype(jnp.bfloat16)
    return (layer_out, new_matrix, new_normal, new_stable)
```

```python
import functools

import jax
import jax.numpy as jnp
from jax import lax
from jax.experimental import pallas as pl
from jax.experimental.pallas import tpu as pltpu
from jax.sharding import PartitionSpec as P

D = 4096
HEADS = 16
DQK = 128
DV = 256
PROP = 4
LANES = 128
HALF = 64
NEG = -1e30
F32 = jnp.float32
BF16 = jnp.bfloat16
HP = lax.Precision.HIGHEST


def ancestry(parents):
    count = parents.shape[1]
    index = jnp.arange(count, dtype=jnp.int32)
    current = jnp.broadcast_to(index[None, :], parents.shape)
    table = jnp.broadcast_to(
        (index[:, None] == index[None, :]).astype(F32), (parents.shape[0], count, count)
    )
    for repeat in range(count - 1):
        hit = current[:, :, None] == index[None, None, :]
        looked = jnp.sum(jnp.where(hit, parents[:, None, :], 0), axis=2)
        current = jnp.where(current >= 0, looked, -1)
        table = table + (current[:, :, None] == index[None, None, :]).astype(F32)
    return table


def split_halves(full):
    lane = lax.broadcasted_iota(jnp.int32, full.shape, full.ndim - 1)
    lead = full.astype(BF16)
    rest = (full - lead.astype(F32)).astype(BF16)
    return jnp.where(lane < HALF, lead.astype(F32), rest.astype(F32)).astype(BF16)


def proj_kernel(with_gates, sq_lane, *refs):
    idx_ref, tok_ref, gain_ref = refs[:3]
    weights = refs[3:-1]
    out_ref = refs[-1]
    x = tok_ref[...].astype(F32)
    normed = (x * gain_ref[...]).astype(BF16)
    at = 0
    for n, w_ref in enumerate(weights):
        width = w_ref.shape[1]
        prod = jnp.dot(normed, w_ref[...], preferred_element_type=F32)
        if with_gates and n == 0:
            squares = jnp.sum(x * x, axis=1, keepdims=True)
            lane = lax.broadcasted_iota(jnp.int32, prod.shape, 1)
            full = jnp.where(lax.rem(lane, HALF) == sq_lane, squares, prod)
            out_ref[0, :, at : at + width] = split_halves(full)
        else:
            out_ref[0, :, at : at + width] = prod.astype(BF16)
        at += width


def project(idx, tokens, gain, weights, rows, with_gates, sq_lane):
    blocks = idx.shape[0]
    depth = tokens.shape[1]
    total = sum(w.shape[1] for w in weights)
    return pl.pallas_call(
        functools.partial(proj_kernel, with_gates, sq_lane),
        out_shape=jax.ShapeDtypeStruct((blocks, rows, total), BF16),
        grid_spec=pltpu.PrefetchScalarGridSpec(
            num_scalar_prefetch=1,
            grid=(blocks,),
            in_specs=[
                pl.BlockSpec((rows, depth), lambda i, idx: (idx[i], 0)),
                pl.BlockSpec((1, depth), lambda i, idx: (0, 0)),
            ]
            + [pl.BlockSpec(w.shape, lambda i, idx: (0, 0)) for w in weights],
            out_specs=pl.BlockSpec((1, rows, total), lambda i, idx: (i, 0, 0)),
        ),
        cost_estimate=pl.CostEstimate(
            flops=2 * blocks * rows * depth * total,
            bytes_accessed=2 * depth * total + 2 * blocks * rows * total,
            transcendentals=0,
        ),
        name="project",
    )(idx, tokens, gain, *weights)


def combine_kernel(count, with_gates, *refs):
    ins = refs[:count]
    outs = refs[count:]
    for b, out_ref in enumerate(outs):
        acc = ins[0][b].astype(F32)
        for other in ins[1:]:
            acc = acc + other[b].astype(F32)
        if with_gates:
            gates = acc[:, :LANES]
            gates = gates + pltpu.roll(gates, HALF, 1)
            out_ref[:, :LANES] = split_halves(gates)
            out_ref[:, LANES:] = acc[:, LANES:].astype(BF16)
        else:
            out_ref[...] = acc.astype(BF16)


def combine(parts, with_gates):
    blocks, rows, width = parts[0].shape
    vmem = pl.BlockSpec(memory_space=pltpu.VMEM)
    return pl.pallas_call(
        functools.partial(combine_kernel, len(parts), with_gates),
        out_shape=[jax.ShapeDtypeStruct((rows, width), BF16)] * blocks,
        in_specs=[vmem] * len(parts),
        out_specs=[vmem] * blocks,
        cost_estimate=pl.CostEstimate(
            flops=0,
            bytes_accessed=2 * (len(parts) + 1) * blocks * rows * width,
            transcendentals=0,
        ),
        name="combine",
    )(*parts)


def commit_kernel(seqs, heads, decay_ref, m_ref, k_ref, v_ref, w_ref, out_ref, low_ref):
    step = pl.program_id(0)
    rows = seqs * PROP
    row_seq = lax.broadcasted_iota(jnp.int32, (rows, 1), 0) // PROP
    for h in range(heads):
        keys = k_ref[:, h * DQK : (h + 1) * DQK].astype(F32)
        vals = v_ref[:, h * DV : (h + 1) * DV].astype(F32) * w_ref[:, h : h + 1]
        lead = vals.astype(BF16)
        rest = (vals - lead.astype(F32)).astype(BF16)
        both = jnp.concatenate([lead, rest], axis=0)
        for s in range(seqs):
            own = jnp.where(row_seq == s, keys, 0.0).astype(BF16)
            added = lax.dot_general(
                jnp.concatenate([own, own], axis=0),
                both,
                (((0,), (0,)), ((), ())),
                preferred_element_type=F32,
            )
            new = decay_ref[step * seqs + s, h] * m_ref[s, h] + added
            out_ref[s, h] = new
            low_ref[s, h] = new.astype(BF16)


def commit_matrix(decay, matrix, keys, values, weights, seqs):
    total, heads, _, _ = matrix.shape
    rows = seqs * PROP
    block = pl.BlockSpec((seqs, heads, DQK, DV), lambda i: (i, 0, 0, 0))
    return pl.pallas_call(
        functools.partial(commit_kernel, seqs, heads),
        grid=(total // seqs,),
        out_shape=[
            jax.ShapeDtypeStruct(matrix.shape, F32),
            jax.ShapeDtypeStruct(matrix.shape, BF16),
        ],
        in_specs=[
            pl.BlockSpec(memory_space=pltpu.SMEM),
            block,
            pl.BlockSpec((rows, heads * DQK), lambda i: (i, 0)),
            pl.BlockSpec((rows, heads * DV), lambda i: (i, 0)),
            pl.BlockSpec((rows, LANES), lambda i: (i, 0)),
        ],
        out_specs=[block, block],
        cost_estimate=pl.CostEstimate(
            flops=2 * matrix.size * 8, bytes_accessed=matrix.size * 10, transcendentals=0
        ),
        name="commit",
    )(decay, matrix, keys, values, weights)


def read_kernel(heads, ny, nz, *refs):
    first = refs[:nz]
    second = refs[nz : nz + ny]
    m_ref, table_ref, stable_ref, normal_ref, bias_ref, gain_ref, out_ref = refs[nz + ny :]
    rows = out_ref.shape[0]
    one = first[0][...].astype(F32)
    for r in first[1:]:
        one = one + r[...].astype(F32)
    two = second[0][...].astype(F32)
    for r in second[1:]:
        two = two + r[...].astype(F32)
    gates = one[:, :LANES]
    gates = gates + pltpu.roll(gates, HALF, 1)
    scale = lax.rsqrt(gates[:, 2 * heads : 2 * heads + 1] * (1.0 / D) + 1e-06)
    gates = scale * gates
    x = gates + bias_ref[...]
    logforget = jnp.minimum(x, 0.0) - jnp.log1p(jnp.exp(-jnp.abs(x)))
    table = table_ref[...]
    path = jnp.dot(table, logforget, precision=HP, preferred_element_type=F32)
    lifted = pltpu.roll(gates, heads, 1) - path
    pick = (
        lax.broadcasted_iota(jnp.int32, (8, LANES), 1)
        == lax.broadcasted_iota(jnp.int32, (8, LANES), 0) + heads
    ).astype(F32)
    flat = lax.dot_general(
        pick, lifted, (((1,), (1,)), ((), ())), precision=HP, preferred_element_type=F32
    )
    carried_all = path + stable_ref[...]
    row16 = lax.broadcasted_iota(jnp.int32, (16, 1), 0) // PROP
    key_scale = scale / jnp.sqrt(jnp.float32(DQK))
    at_value = LANES + heads * DQK
    at_gate = heads * DQK
    for h in range(heads):
        query = scale * one[:, LANES + h * DQK : LANES + (h + 1) * DQK]
        value = scale * one[:, at_value + h * DV : at_value + (h + 1) * DV]
        key = key_scale * two[:, h * DQK : (h + 1) * DQK]
        outgate = scale * two[:, at_gate + h * DV : at_gate + (h + 1) * DV]
        dlog = path[:, heads + h : heads + h + 1] + flat[h : h + 1, :]
        dlog = jnp.where(table > 0.5, dlog, NEG)
        carried = carried_all[:, heads + h : heads + h + 1]
        top = jnp.maximum(carried, jnp.max(dlog, axis=1, keepdims=True))
        scores = lax.dot_general(
            query, key, (((1,), (1,)), ((), ())), precision=HP, preferred_element_type=F32
        ) * jnp.exp(dlog - top)
        factor = jnp.exp(carried - top)
        low = query.astype(BF16)
        pieces = []
        for g in range(rows // 16):
            part = low[g * 16 : (g + 1) * 16]
            got = None
            for j in range(16 // PROP):
                res = jnp.dot(
                    part, m_ref[g * (16 // PROP) + j, h], preferred_element_type=F32
                )
                got = res if got is None else jnp.where(row16 == j, res, got)
            pieces.append(got)
        from_state = jnp.concatenate(pieces, axis=0)
        numer = (
            jnp.dot(scores, value, precision=HP, preferred_element_type=F32)
            + factor * from_state
        )
        denom = jnp.sum(scores, axis=1, keepdims=True) + factor * jnp.sum(
            query * normal_ref[:, h * DQK : (h + 1) * DQK], axis=1, keepdims=True
        )
        read = numer / jnp.maximum(jnp.abs(denom), jnp.exp(-top))
        normer = lax.rsqrt(jnp.mean(read * read, axis=1, keepdims=True) + 1e-06)
        hidden = (
            read
            * normer
            * gain_ref[:, h * DV : (h + 1) * DV]
            * (1.0 / (1.0 + jnp.exp(-outgate)))
        )
        out_ref[:, h * DV : (h + 1) * DV] = hidden.astype(BF16)


def tree_read(first, second, matrix, table, stable, normal, bias, gain, rows):
    heads = matrix.shape[1]
    total = first[0].shape[0]
    seqs = rows // PROP

    def by_row(a):
        return pl.BlockSpec((rows, a.shape[1]), lambda i: (i, 0))

    def whole(a):
        return pl.BlockSpec(a.shape, lambda i: (0, 0))

    return pl.pallas_call(
        functools.partial(read_kernel, heads, len(second), len(first)),
        grid=(total // rows,),
        out_shape=jax.ShapeDtypeStruct((total, heads * DV), BF16),
        in_specs=[by_row(a) for a in first]
        + [by_row(a) for a in second]
        + [
            pl.BlockSpec((seqs, heads, DQK, DV), lambda i: (i, 0, 0, 0)),
            pl.BlockSpec((rows, rows), lambda i: (i, 0)),
            by_row(stable),
            by_row(normal),
            whole(bias),
            whole(gain),
        ],
        out_specs=pl.BlockSpec((rows, heads * DV), lambda i: (i, 0)),
        cost_estimate=pl.CostEstimate(
            flops=8 * matrix.size, bytes_accessed=matrix.size * 2, transcendentals=0
        ),
        name="tree_read",
    )(*first, *second, matrix, table, stable, normal, bias, gain)


def remote(src, dst, send_sem, recv_sem, kv_index, tp_index):
    return pltpu.make_async_remote_copy(
        src_ref=src,
        dst_ref=dst,
        send_sem=send_sem,
        recv_sem=recv_sem,
        device_id=(kv_index, tp_index),
        device_id_type=pl.DeviceIdType.MESH,
    )


def greet(others):
    barrier = pltpu.get_barrier_semaphore()
    for other in others:
        pl.semaphore_signal(
            barrier, inc=1, device_id=other, device_id_type=pl.DeviceIdType.MESH
        )
    pl.semaphore_wait(barrier, len(others))


def spread_kernel(
    ny, nz, tp, cuts, hid_ref, w_ref, out_ref, held, parts, landed, total,
    up_sem, down_sem, side_sem, got_sem, part_sem, land_sem,
):
    me = lax.axis_index("kv")
    mine = lax.axis_index("tp")
    z, y = me // ny, lax.rem(me, ny)
    kv = ny * nz
    per = kv // tp
    rows = hid_ref.shape[0]
    piece = rows // cuts
    greet(
        [((z + d) % nz * ny + y, mine) for d in sorted({1 % nz, nz - 1}) if d]
        + [(z * ny + (y + d) % ny, mine) for d in range(1, ny)]
        + [(me, (mine + d) % tp) for d in range(1, tp)]
    )

    def slab(b, c):
        return held.at[b, pl.ds(c * piece, piece)]

    def source(s, b, c):
        return hid_ref.at[pl.ds(c * piece, piece)] if s == 0 else slab(b, c)

    def up(s, b, c):
        return remote(source(s, b, c), slab(b, c), up_sem.at[s, c], got_sem.at[b, c], me + ny, mine)

    def down(s, b, c):
        return remote(source(s, b, c), slab(b, c), down_sem.at[s, c], got_sem.at[b, c], me - ny, mine)

    def side(s, b, c, d, way):
        return remote(
            source(s, b, c), slab(b, c), side_sem.at[way, s, d - 1, c], got_sem.at[b, c],
            z * ny + (y + d) % ny, mine,
        )

    def arrive(b, c):
        return remote(slab(b, c), slab(b, c), part_sem.at[b], got_sem.at[b, c], me, mine)

    def product(s, b):
        value = hid_ref[...] if s == 0 else held[b]
        got = jnp.dot(value, w_ref[...], preferred_element_type=F32)
        owner = b // per
        slot = b % per

        @pl.when(owner == mine)
        def _():
            total[slot] = got

        @pl.when(owner != mine)
        def _():
            parts[b] = got.astype(BF16)
            hand(b).start()

    def hand(b):
        owner = b // per
        slot = ((mine + tp - owner) % tp + tp - 1) % tp * per + b % per
        return remote(parts.at[b], landed.at[slot], part_sem.at[b], land_sem.at[slot], me, owner)

    for c in range(cuts):
        @pl.when(z < nz - 1)
        def _():
            up(0, me, c).start()

        @pl.when(z > 0)
        def _():
            down(0, me, c).start()

        for d in range(1, ny):
            side(0, me, c, d, 0).start()
    product(0, me)

    def from_side(s, way):
        base = (z - s + nz) % nz * ny if way == 0 else (z + s) % nz * ny
        for d in range(1, ny):
            b = base + (y + d) % ny
            for c in range(cuts):
                arrive(b, c).wait_recv()
            product(1, b)

    def ways(s):
        return [(0, z - s >= 0)] if s == 0 else [(0, z - s >= 0), (1, z + s < nz)]

    for s in range(1, nz):
        for way, there in ways(s):
            b = ((z - s + nz) % nz if way == 0 else (z + s) % nz) * ny + y

            @pl.when(there)
            def _():
                for c in range(cuts):
                    arrive(b, c).wait_recv()
                    if s < nz - 1:
                        if way == 0:
                            @pl.when(z < nz - 1)
                            def _():
                                up(s, b, c).start()
                        else:
                            @pl.when(z > 0)
                            def _():
                                down(s, b, c).start()
                    for d in range(1, ny):
                        side(s, b, c, d, way).start()
                product(s, b)

        for way, there in ways(s - 1):
            @pl.when(there)
            def _():
                from_side(s - 1, way)

    for way, there in ways(nz - 1):
        @pl.when(there)
        def _():
            from_side(nz - 1, way)

    for slot in range(per):
        acc = total[slot]
        for d in range(1, tp):
            at = (d - 1) * per + slot
            remote(landed.at[at], landed.at[at], part_sem.at[0], land_sem.at[at], me, mine).wait_recv()
            acc = acc + landed[at].astype(F32)
        out_ref[slot * rows : (slot + 1) * rows] = acc.astype(BF16)

    for s in range(nz):
        for way, there in ways(s):
            b = ((z - s + nz) % nz if way == 0 else (z + s) % nz) * ny + y

            @pl.when(there)
            def _():
                for c in range(cuts):
                    if s < nz - 1:
                        if way == 0:
                            @pl.when(z < nz - 1)
                            def _():
                                up(s, b, c).wait_send()
                        if way == 1 or s == 0:
                            @pl.when(z > 0)
                            def _():
                                down(s, b, c).wait_send()
                    for d in range(1, ny):
                        side(s, b, c, d, way).wait_send()
    for b in range(kv):
        @pl.when(b // per != mine)
        def _():
            hand(b).wait_send()


def spread_out(hidden, weight, ny, nz, tp):
    rows, width = hidden.shape
    cols = weight.shape[1]
    kv = ny * nz
    per = kv // tp
    cuts = 2
    vmem = pl.BlockSpec(memory_space=pltpu.VMEM)
    dma = pltpu.SemaphoreType.DMA
    return pl.pallas_call(
        functools.partial(spread_kernel, ny, nz, tp, cuts),
        out_shape=jax.ShapeDtypeStruct((per * rows, cols), BF16),
        in_specs=[vmem, vmem],
        out_specs=vmem,
        scratch_shapes=[
            pltpu.VMEM((kv, rows, width), BF16),
            pltpu.VMEM((kv, rows, cols), BF16),
            pltpu.VMEM(((tp - 1) * per, rows, cols), BF16),
            pltpu.VMEM((per, rows, cols), F32),
            dma((nz, cuts)),
            dma((nz, cuts)),
            dma((2, nz, max(ny - 1, 1), cuts)),
            dma((kv, cuts)),
            dma((kv,)),
            dma(((tp - 1) * per,)),
        ],
        compiler_params=pltpu.CompilerParams(collective_id=0, has_side_effects=True),
        cost_estimate=pl.CostEstimate(
            flops=2 * kv * rows * width * cols, bytes_accessed=8 * rows * width, transcendentals=0
        ),
        name="spread",
    )(hidden, weight)


def per_device(
    kv,
    tp,
    tokens,
    norm_gain,
    query_weight,
    key_weight,
    value_weight,
    outgate_weight,
    gate_weight,
    forget_bias,
    head_gain,
    output_weight,
    state_matrix,
    state_normal,
    state_stable,
    prior_keys,
    prior_values,
    prior_ingate,
    prior_forget,
    accepted,
    parents,
):
    ny = 1 << ((kv.bit_length() - 1) // 2)
    nz = kv // ny
    me = lax.axis_index("kv")
    mine = lax.axis_index("tp")
    z, y = me // ny, lax.rem(me, ny)
    heads = query_weight.shape[1] // DQK
    depth = tokens.shape[1]
    seqs = accepted.shape[0]
    rows = seqs * PROP

    def over_y(a, d):
        return lax.ppermute(
            a, "kv", [(p * ny + q, p * ny + (q + d) % ny) for p in range(nz) for q in range(ny)]
        )

    def over_z(a, d):
        return lax.ppermute(
            a, "kv", [(p * ny + q, (p + d) % nz * ny + q) for p in range(nz) for q in range(ny)]
        )

    own_gain = lax.dynamic_slice_in_dim(norm_gain, me * depth, depth, 0)[None, :]
    head_start = mine * heads
    picked = lax.dynamic_slice_in_dim(
        gate_weight.reshape(depth, 2, HEADS), head_start, heads, 2
    ).reshape(depth, 2 * heads)
    half_gate = jnp.pad(picked, ((0, 0), (0, HALF - 2 * heads)))
    gate_cols = jnp.concatenate([half_gate, half_gate], axis=1)
    y_first = (gate_cols, query_weight, value_weight)
    z_first = (key_weight, outgate_weight)

    def y_part(d):
        zz = lax.rem(z + jnp.arange(nz, dtype=jnp.int32), nz)
        idx = zz * ny + lax.rem(y + d, ny)
        return project(idx, tokens, own_gain, y_first, rows, True, 2 * heads)

    def z_part(d):
        yy = lax.rem(y + jnp.arange(ny, dtype=jnp.int32), ny)
        idx = lax.rem(z + d, nz) * ny + yy
        return project(idx, tokens, own_gain, z_first, rows, False, 0)

    y_got = [over_y(y_part(d), d) for d in range(1, ny)]
    z_got = [over_z(z_part(d), d) for d in range(1, nz)]
    y_own = y_part(0)
    z_own = z_part(0)

    live = (jnp.arange(PROP, dtype=jnp.int32)[None, :] < accepted[:, None])[:, :, None]
    forget_live = jnp.where(live, prior_forget, 0.0)
    cumul = [forget_live[:, 0]]
    for p in range(1, PROP):
        cumul.append(cumul[-1] + forget_live[:, p])
    total = cumul[-1]
    cumul = jnp.stack(cumul, axis=1)
    weight_log = jnp.where(live, total[:, None, :] - cumul + prior_ingate, -jnp.inf)
    new_stable = jnp.maximum(total + state_stable, jnp.max(weight_log, axis=1))
    weights = jnp.exp(weight_log - new_stable[:, None, :])
    decay = jnp.exp(total + state_stable - new_stable)
    new_normal = decay[:, :, None] * state_normal + jnp.sum(
        weights[..., None] * prior_keys.astype(F32).reshape(seqs, PROP, heads, DQK), axis=1
    )
    weight_rows = jnp.pad(weights.reshape(rows, heads), ((0, 0), (0, LANES - heads)))
    new_matrix, low_matrix = commit_matrix(
        decay,
        state_matrix,
        prior_keys.reshape(rows, heads * DQK),
        prior_values.reshape(rows, heads * DV),
        weight_rows,
        4,
    )

    step_rows = 32
    group = step_rows // PROP
    table = ancestry(parents)
    spread = (
        table.reshape(seqs // group, group, PROP, 1, PROP)
        * jnp.eye(group, dtype=F32)[None, :, None, :, None]
    ).reshape(rows, step_rows)
    stable_rows = jnp.pad(
        jnp.repeat(new_stable, PROP, axis=0), ((0, 0), (heads, LANES - 2 * heads))
    )
    normal_rows = jnp.repeat(new_normal.reshape(seqs, heads * DQK), PROP, axis=0)
    bias = jnp.pad(
        lax.dynamic_slice_in_dim(forget_bias, head_start, heads, 0), (heads, LANES - 2 * heads)
    )[None, :]

    y_own, z_own, low_matrix = lax.optimization_barrier((y_own, z_own, low_matrix))
    y_sums = combine([y_own] + y_got, True)
    first = [y_sums[0]] + [over_z(y_sums[d], d) for d in range(1, nz)]
    z_sums = combine([z_own] + z_got, False)
    second = [z_sums[0]] + [over_y(z_sums[d], d) for d in range(1, ny)]

    hidden = tree_read(
        first,
        second,
        low_matrix,
        spread,
        stable_rows,
        normal_rows,
        bias,
        head_gain[None, :],
        step_rows,
    )

    layer_out = spread_out(hidden, output_weight, ny, nz, tp)
    return (layer_out, new_matrix, new_normal, new_stable)


def solution(mesh):
    placed = (
        P(None, "kv"),
        P(),
        P("kv", "tp"),
        P("kv", "tp"),
        P("kv", "tp"),
        P("kv", "tp"),
        P("kv", None),
        P(),
        P("tp"),
        P("tp", "kv"),
        P("kv", "tp", None, None),
        P("kv", "tp", None),
        P("kv", "tp"),
        P("kv", None, "tp"),
        P("kv", None, "tp"),
        P("kv", None, "tp"),
        P("kv", None, "tp"),
        P("kv"),
        P("kv", None),
    )
    return jax.shard_map(
        functools.partial(per_device, mesh.shape["kv"], mesh.shape["tp"]),
        mesh=mesh,
        in_specs=placed,
        out_specs=(P("tp", "kv"), P("kv", "tp", None, None), P("kv", "tp", None), P("kv", "tp")),
        check_vma=False,
    )
```

```python
import functools

import jax
import jax.numpy as jnp
from jax import lax
from jax.experimental import pallas as pl
from jax.experimental.pallas import tpu as pltpu
from jax.sharding import PartitionSpec as P

D = 4096
HEADS = 16
DQK = 128
DV = 256
PROP = 4
LANES = 128
NEG = -1e30
F32 = jnp.float32
BF16 = jnp.bfloat16
HP = lax.Precision.HIGHEST


def ancestry(parents):
    count = parents.shape[1]
    index = jnp.arange(count, dtype=jnp.int32)
    current = jnp.broadcast_to(index[None, :], parents.shape)
    table = jnp.broadcast_to(
        (index[:, None] == index[None, :]).astype(F32), (parents.shape[0], count, count)
    )
    for repeat in range(count - 1):
        hit = current[:, :, None] == index[None, None, :]
        looked = jnp.sum(jnp.where(hit, parents[:, None, :], 0), axis=2)
        current = jnp.where(current >= 0, looked, -1)
        table = table + (current[:, :, None] == index[None, None, :]).astype(F32)
    return table


def commit_kernel(seqs, heads, decay_ref, m_ref, k_ref, v_ref, w_ref, out_ref, low_ref):
    step = pl.program_id(0)
    rows = seqs * PROP
    row_seq = lax.broadcasted_iota(jnp.int32, (rows, 1), 0) // PROP
    for h in range(heads):
        keys = k_ref[:, h * DQK : (h + 1) * DQK].astype(F32)
        vals = v_ref[:, h * DV : (h + 1) * DV].astype(F32) * w_ref[:, h : h + 1]
        lead = vals.astype(BF16)
        rest = (vals - lead.astype(F32)).astype(BF16)
        both = jnp.concatenate([lead, rest], axis=0)
        for s in range(seqs):
            own = jnp.where(row_seq == s, keys, 0.0).astype(BF16)
            added = lax.dot_general(
                jnp.concatenate([own, own], axis=0),
                both,
                (((0,), (0,)), ((), ())),
                preferred_element_type=F32,
            )
            new = decay_ref[step * seqs + s, h] * m_ref[s, h] + added
            out_ref[s, h] = new
            low_ref[s, h] = new.astype(BF16)


def commit_matrix(decay, matrix, keys, values, weights, seqs):
    total, heads, _, _ = matrix.shape
    rows = seqs * PROP
    block = pl.BlockSpec((seqs, heads, DQK, DV), lambda i: (i, 0, 0, 0))
    return pl.pallas_call(
        functools.partial(commit_kernel, seqs, heads),
        grid=(total // seqs,),
        out_shape=[
            jax.ShapeDtypeStruct(matrix.shape, F32),
            jax.ShapeDtypeStruct(matrix.shape, BF16),
        ],
        in_specs=[
            pl.BlockSpec(memory_space=pltpu.SMEM),
            block,
            pl.BlockSpec((rows, heads * DQK), lambda i: (i, 0)),
            pl.BlockSpec((rows, heads * DV), lambda i: (i, 0)),
            pl.BlockSpec((rows, LANES), lambda i: (i, 0)),
        ],
        out_specs=[block, block],
        cost_estimate=pl.CostEstimate(
            flops=2 * matrix.size * 8, bytes_accessed=matrix.size * 10, transcendentals=0
        ),
        name="commit",
    )(decay, matrix, keys, values, weights)


def read_kernel(
    heads, sq_lane, q_ref, rest_ref, gates_ref, m_ref, table_ref, stable_ref, normal_ref,
    bias_ref, gain_ref, out_ref,
):
    rows = out_ref.shape[0]
    gates = gates_ref[...]
    scale = lax.rsqrt(gates[:, sq_lane : sq_lane + 1] * (1.0 / D) + 1e-06)
    gates = scale * gates
    x = gates + bias_ref[...]
    logforget = jnp.minimum(x, 0.0) - jnp.log1p(jnp.exp(-jnp.abs(x)))
    table = table_ref[...]
    path = jnp.dot(table, logforget, precision=HP, preferred_element_type=F32)
    lifted = pltpu.roll(gates, heads, 1) - path
    pick = (
        lax.broadcasted_iota(jnp.int32, (8, LANES), 1)
        == lax.broadcasted_iota(jnp.int32, (8, LANES), 0) + heads
    ).astype(F32)
    flat = lax.dot_general(
        pick, lifted, (((1,), (1,)), ((), ())), precision=HP, preferred_element_type=F32
    )
    carried_all = path + stable_ref[...]
    row16 = lax.broadcasted_iota(jnp.int32, (16, 1), 0) // PROP
    key_scale = scale / jnp.sqrt(jnp.float32(DQK))
    at_value = heads * DQK
    at_gate = at_value + heads * DV
    for h in range(heads):
        query = scale * q_ref[:, h * DQK : (h + 1) * DQK]
        value = scale * rest_ref[:, at_value + h * DV : at_value + (h + 1) * DV]
        key = key_scale * rest_ref[:, h * DQK : (h + 1) * DQK]
        outgate = scale * rest_ref[:, at_gate + h * DV : at_gate + (h + 1) * DV]
        dlog = path[:, heads + h : heads + h + 1] + flat[h : h + 1, :]
        dlog = jnp.where(table > 0.5, dlog, NEG)
        carried = carried_all[:, heads + h : heads + h + 1]
        top = jnp.maximum(carried, jnp.max(dlog, axis=1, keepdims=True))
        scores = lax.dot_general(
            query, key, (((1,), (1,)), ((), ())), precision=HP, preferred_element_type=F32
        ) * jnp.exp(dlog - top)
        factor = jnp.exp(carried - top)
        low = query.astype(BF16)
        pieces = []
        for g in range(rows // 16):
            part = low[g * 16 : (g + 1) * 16]
            got = None
            for j in range(16 // PROP):
                res = jnp.dot(
                    part, m_ref[g * (16 // PROP) + j, h], preferred_element_type=F32
                )
                got = res if got is None else jnp.where(row16 == j, res, got)
            pieces.append(got)
        from_state = jnp.concatenate(pieces, axis=0)
        numer = (
            jnp.dot(scores, value, precision=HP, preferred_element_type=F32)
            + factor * from_state
        )
        denom = jnp.sum(scores, axis=1, keepdims=True) + factor * jnp.sum(
            query * normal_ref[:, h * DQK : (h + 1) * DQK], axis=1, keepdims=True
        )
        read = numer / jnp.maximum(jnp.abs(denom), jnp.exp(-top))
        normer = lax.rsqrt(jnp.mean(read * read, axis=1, keepdims=True) + 1e-06)
        hidden = (
            read
            * normer
            * gain_ref[:, h * DV : (h + 1) * DV]
            * (1.0 / (1.0 + jnp.exp(-outgate)))
        )
        out_ref[:, h * DV : (h + 1) * DV] = hidden.astype(BF16)


def tree_read(query, rest, gates, sq_lane, matrix, table, stable, normal, bias, gain, rows):
    heads = matrix.shape[1]
    total = query.shape[0]
    seqs = rows // PROP

    def by_row(a):
        return pl.BlockSpec((rows, a.shape[1]), lambda i: (i, 0))

    def whole(a):
        return pl.BlockSpec(a.shape, lambda i: (0, 0))

    return pl.pallas_call(
        functools.partial(read_kernel, heads, sq_lane),
        grid=(total // rows,),
        out_shape=jax.ShapeDtypeStruct((total, heads * DV), BF16),
        in_specs=[by_row(a) for a in (query, rest, gates)]
        + [
            pl.BlockSpec((seqs, heads, DQK, DV), lambda i: (i, 0, 0, 0)),
            pl.BlockSpec((rows, rows), lambda i: (i, 0)),
            by_row(stable),
            by_row(normal),
            whole(bias),
            whole(gain),
        ],
        out_specs=pl.BlockSpec((rows, heads * DV), lambda i: (i, 0)),
        cost_estimate=pl.CostEstimate(
            flops=8 * matrix.size, bytes_accessed=matrix.size * 2, transcendentals=0
        ),
        name="tree_read",
    )(query, rest, gates, matrix, table, stable, normal, bias, gain)


def remote(src, dst, send_sem, recv_sem, kv_index, tp_index):
    return pltpu.make_async_remote_copy(
        src_ref=src,
        dst_ref=dst,
        send_sem=send_sem,
        recv_sem=recv_sem,
        device_id=(kv_index, tp_index),
        device_id_type=pl.DeviceIdType.MESH,
    )


def greet(others):
    barrier = pltpu.get_barrier_semaphore()
    for other in others:
        pl.semaphore_signal(
            barrier, inc=1, device_id=other, device_id_type=pl.DeviceIdType.MESH
        )
    pl.semaphore_wait(barrier, len(others))


def spread_kernel(
    ny, nz, tp, cuts, hid_ref, w_ref, out_ref, held, parts, landed, total,
    up_sem, down_sem, side_sem, got_sem, part_sem, land_sem,
):
    me = lax.axis_index("kv")
    mine = lax.axis_index("tp")
    z, y = me // ny, lax.rem(me, ny)
    kv = ny * nz
    per = kv // tp
    rows = hid_ref.shape[0]
    piece = rows // cuts
    greet(
        [((z + d) % nz * ny + y, mine) for d in sorted({1 % nz, nz - 1}) if d]
        + [(z * ny + (y + d) % ny, mine) for d in range(1, ny)]
        + [(me, (mine + d) % tp) for d in range(1, tp)]
    )

    def slab(b, c):
        return held.at[b, pl.ds(c * piece, piece)]

    def source(s, b, c):
        return hid_ref.at[pl.ds(c * piece, piece)] if s == 0 else slab(b, c)

    def up(s, b, c):
        return remote(source(s, b, c), slab(b, c), up_sem.at[s, c], got_sem.at[b, c], me + ny, mine)

    def down(s, b, c):
        return remote(source(s, b, c), slab(b, c), down_sem.at[s, c], got_sem.at[b, c], me - ny, mine)

    def side(s, b, c, d, way):
        return remote(
            source(s, b, c), slab(b, c), side_sem.at[way, s, d - 1, c], got_sem.at[b, c],
            z * ny + (y + d) % ny, mine,
        )

    def arrive(b, c):
        return remote(slab(b, c), slab(b, c), part_sem.at[b], got_sem.at[b, c], me, mine)

    def product(s, b):
        value = hid_ref[...] if s == 0 else held[b]
        got = jnp.dot(value, w_ref[...], preferred_element_type=F32)
        owner = b // per
        slot = b % per

        @pl.when(owner == mine)
        def _():
            total[slot] = got

        @pl.when(owner != mine)
        def _():
            parts[b] = got.astype(BF16)
            hand(b).start()

    def hand(b):
        owner = b // per
        slot = ((mine + tp - owner) % tp + tp - 1) % tp * per + b % per
        return remote(parts.at[b], landed.at[slot], part_sem.at[b], land_sem.at[slot], me, owner)

    for c in range(cuts):
        @pl.when(z < nz - 1)
        def _():
            up(0, me, c).start()

        @pl.when(z > 0)
        def _():
            down(0, me, c).start()

        for d in range(1, ny):
            side(0, me, c, d, 0).start()
    product(0, me)

    def from_side(s, way):
        base = (z - s + nz) % nz * ny if way == 0 else (z + s) % nz * ny
        for d in range(1, ny):
            b = base + (y + d) % ny
            for c in range(cuts):
                arrive(b, c).wait_recv()
            product(1, b)

    def ways(s):
        return [(0, z - s >= 0)] if s == 0 else [(0, z - s >= 0), (1, z + s < nz)]

    for s in range(1, nz):
        for way, there in ways(s):
            b = ((z - s + nz) % nz if way == 0 else (z + s) % nz) * ny + y

            @pl.when(there)
            def _():
                for c in range(cuts):
                    arrive(b, c).wait_recv()
                    if s < nz - 1:
                        if way == 0:
                            @pl.when(z < nz - 1)
                            def _():
                                up(s, b, c).start()
                        else:
                            @pl.when(z > 0)
                            def _():
                                down(s, b, c).start()
                    for d in range(1, ny):
                        side(s, b, c, d, way).start()
                product(s, b)

        for way, there in ways(s - 1):
            @pl.when(there)
            def _():
                from_side(s - 1, way)

    for way, there in ways(nz - 1):
        @pl.when(there)
        def _():
            from_side(nz - 1, way)

    for slot in range(per):
        acc = total[slot]
        for d in range(1, tp):
            at = (d - 1) * per + slot
            remote(landed.at[at], landed.at[at], part_sem.at[0], land_sem.at[at], me, mine).wait_recv()
            acc = acc + landed[at].astype(F32)
        out_ref[slot * rows : (slot + 1) * rows] = acc.astype(BF16)

    for s in range(nz):
        for way, there in ways(s):
            b = ((z - s + nz) % nz if way == 0 else (z + s) % nz) * ny + y

            @pl.when(there)
            def _():
                for c in range(cuts):
                    if s < nz - 1:
                        if way == 0:
                            @pl.when(z < nz - 1)
                            def _():
                                up(s, b, c).wait_send()
                        if way == 1 or s == 0:
                            @pl.when(z > 0)
                            def _():
                                down(s, b, c).wait_send()
                    for d in range(1, ny):
                        side(s, b, c, d, way).wait_send()
    for b in range(kv):
        @pl.when(b // per != mine)
        def _():
            hand(b).wait_send()


def spread_out(hidden, weight, ny, nz, tp):
    rows, width = hidden.shape
    cols = weight.shape[1]
    kv = ny * nz
    per = kv // tp
    cuts = 2
    vmem = pl.BlockSpec(memory_space=pltpu.VMEM)
    dma = pltpu.SemaphoreType.DMA
    return pl.pallas_call(
        functools.partial(spread_kernel, ny, nz, tp, cuts),
        out_shape=jax.ShapeDtypeStruct((per * rows, cols), BF16),
        in_specs=[vmem, vmem],
        out_specs=vmem,
        scratch_shapes=[
            pltpu.VMEM((kv, rows, width), BF16),
            pltpu.VMEM((kv, rows, cols), BF16),
            pltpu.VMEM(((tp - 1) * per, rows, cols), BF16),
            pltpu.VMEM((per, rows, cols), F32),
            dma((nz, cuts)),
            dma((nz, cuts)),
            dma((2, nz, max(ny - 1, 1), cuts)),
            dma((kv, cuts)),
            dma((kv,)),
            dma(((tp - 1) * per,)),
        ],
        compiler_params=pltpu.CompilerParams(collective_id=0, has_side_effects=True),
        cost_estimate=pl.CostEstimate(
            flops=2 * kv * rows * width * cols, bytes_accessed=8 * rows * width, transcendentals=0
        ),
        name="spread",
    )(hidden, weight)


def gather_sums_kernel(
    ny, nz, lag, tok_hbm, gain_ref, gate_ref, q_hbm, k_hbm, v_hbm, o_hbm,
    q_out, rest_out, gates_out,
    tok, normed, wq, wrest, flat,
    side_out, side_in, line_out, below, above, last_out, last_in,
    flat_out, flat_below, flat_above, flat_last_out, flat_last_in,
    load_sem, side_sem, side_got, line_sem, below_got, above_got, last_sem, last_got,
    fline_sem, fbelow_got, fabove_got, flast_sem, flast_got,
):
    me = lax.axis_index("kv")
    mine = lax.axis_index("tp")
    z, y = me // ny, lax.rem(me, ny)
    rows = q_out.shape[0]
    width = wq.shape[1]
    chunks = wrest.shape[0]
    plane = ny * rows
    units = ny + chunks

    loads = [
        pltpu.make_async_copy(tok_hbm, tok, load_sem.at[0]),
        pltpu.make_async_copy(q_hbm, wq, load_sem.at[1]),
    ]
    for n, (w, at) in enumerate(
        [(w, at) for w in (k_hbm, v_hbm, o_hbm) for at in range(0, w.shape[1], width)]
    ):
        loads.append(
            pltpu.make_async_copy(w.at[:, pl.ds(at, width)], wrest.at[n], load_sem.at[2 + n])
        )
    for load in loads:
        load.start()
    greet(
        [((z + d) % nz * ny + y, mine) for d in sorted({1 % nz, nz - 1}) if d]
        + [(z * ny + (y + d) % ny, mine) for d in range(1, ny)]
    )
    loads[0].wait()

    def prepare(n, carry):
        at = pl.ds(pl.multiple_of(n * rows, rows), rows)
        x = tok[at, :].astype(F32)
        low = (x * gain_ref[...]).astype(BF16)
        normed[at, :] = low
        squares = lax.dot_general(
            jnp.ones((8, x.shape[1]), F32), x * x, (((1,), (1,)), ((), ())),
            precision=HP, preferred_element_type=F32,
        )
        gates = lax.dot_general(
            gate_ref[...], low, (((1,), (1,)), ((), ())), preferred_element_type=F32
        )
        flat[n] = jnp.concatenate([gates, squares], axis=0)
        return carry

    lax.fori_loop(0, ny * nz, prepare, 0)
    for load in loads[1:]:
        load.wait()

    def term(block, w):
        at = pl.ds(pl.multiple_of(block * rows, rows), rows)
        return jnp.dot(normed[at, :], w, preferred_element_type=F32)

    def side(d, p, j):
        u = p * chunks + j
        return remote(
            side_out.at[d - 1, u], side_in.at[ny - d - 1, u], side_sem.at[d - 1, u],
            side_got.at[ny - d - 1, u], z * ny + (y + d) % ny, mine,
        )

    def line(going_up, slot):
        got, sem, far = (below, below_got, me + ny) if going_up else (above, above_got, me - ny)
        return remote(line_out.at[slot], got.at[slot], line_sem.at[slot], sem.at[slot], far, mine)

    def flat_line(going_up, b):
        got, sem, far = (
            (flat_below, fbelow_got, me + ny) if going_up else (flat_above, fabove_got, me - ny)
        )
        return remote(flat_out.at[b], got.at[b], fline_sem.at[b], sem.at[b], far, mine)

    def last(d):
        return remote(
            last_out.at[d - 1], last_in.at[ny - d - 1], last_sem.at[d - 1],
            last_got.at[ny - d - 1], z * ny + (y + d) % ny, mine,
        )

    def flat_last(d):
        return remote(
            flat_last_out.at[d - 1], flat_last_in.at[ny - d - 1], flast_sem.at[d - 1],
            flast_got.at[ny - d - 1], z * ny + (y + d) % ny, mine,
        )

    def arrived(ref, sem):
        remote(ref, ref, load_sem.at[0], sem, me, mine).wait_recv()

    def send_side(p, j):
        for d in range(1, ny):
            side_out[d - 1, p * chunks + j] = term(p * ny + (y + d) % ny, wrest[j]).astype(BF16)
            side(d, p, j).start()

    def side_round(n, carry):
        i, j = n // chunks, n % chunks

        @pl.when(nz - 1 - i > z)
        def _():
            send_side(nz - 1 - i, j)

        @pl.when(i < z)
        def _():
            send_side(i, j)

        return carry

    def side_own(j, carry):
        send_side(z, j)
        return carry

    def with_sides(acc, p, j):
        for d in range(1, ny):
            u = p * chunks + j
            arrived(side_in.at[d - 1, u], side_got.at[d - 1, u])
            acc = acc + side_in[d - 1, u].astype(F32)
        return acc

    def pass_on(going_up, acc, slot):
        got, sem = (below, below_got) if going_up else (above, above_got)
        first = z == 0 if going_up else z == nz - 1

        @pl.when(first)
        def _():
            line_out[slot] = acc.astype(BF16)

        @pl.when(jnp.logical_not(first))
        def _():
            arrived(got.at[slot], sem.at[slot])
            line_out[slot] = (acc + got[slot].astype(F32)).astype(BF16)

        line(going_up, slot).start()

    def pass_flat(going_up, b):
        got, sem = (flat_below, fbelow_got) if going_up else (flat_above, fabove_got)
        first = z == 0 if going_up else z == nz - 1

        @pl.when(first)
        def _():
            flat_out[b] = flat[b]

        @pl.when(jnp.logical_not(first))
        def _():
            arrived(got.at[b], sem.at[b])
            flat_out[b] = flat[b] + got[b]

        flat_line(going_up, b).start()

    early = (nz - 1) * ny
    total = early + (nz - 1) * chunks

    def plane_of(going_up, i):
        return nz - 1 - i if going_up else i

    def flow(going_up, n):
        @pl.when(jnp.logical_and(n >= 0, n < early))
        def _():
            p = plane_of(going_up, n // ny)

            @pl.when(p > z if going_up else p < z)
            def _():
                b = p * ny + n % ny
                pass_flat(going_up, b)
                pass_on(going_up, term(b, wq[...]), p * units + n % ny)

        @pl.when(jnp.logical_and(n >= early, n < total))
        def _():
            p = plane_of(going_up, (n - early) // chunks)
            j = (n - early) % chunks

            @pl.when(p > z if going_up else p < z)
            def _():
                pass_on(
                    going_up, with_sides(term(p * ny + y, wrest[j]), p, j), p * units + ny + j
                )

    def close_query():
        for d in range(ny):
            yy = (y + d) % ny
            b, slot = z * ny + yy, z * units + yy
            acc = term(b, wq[...])
            small = flat[b]

            def keep(acc, small):
                if d == 0:
                    q_out[...] = acc
                    flat_out[b] = small
                else:
                    last_out[d - 1] = acc.astype(BF16)
                    flat_last_out[d - 1] = small

            def lower():
                arrived(below.at[slot], below_got.at[slot])
                arrived(flat_below.at[b], fbelow_got.at[b])
                return below[slot].astype(F32), flat_below[b]

            def upper():
                arrived(above.at[slot], above_got.at[slot])
                arrived(flat_above.at[b], fabove_got.at[b])
                return above[slot].astype(F32), flat_above[b]

            @pl.when(z == 0)
            def _():
                more, less = upper()
                keep(acc + more, small + less)

            @pl.when(z == nz - 1)
            def _():
                more, less = lower()
                keep(acc + more, small + less)

            @pl.when(jnp.logical_and(z > 0, z < nz - 1))
            def _():
                more, less = lower()
                again, still = upper()
                keep(acc + more + again, small + less + still)

            if d:
                last(d).start()
                flat_last(d).start()

    lax.fori_loop(0, chunks, side_round, 0)
    close_at = early + lag * (nz - 1) + 1

    def step(n, carry):
        @pl.when(n == 1)
        def _():
            lax.fori_loop(chunks, (nz - 1) * chunks, side_round, 0)
            lax.fori_loop(0, chunks, side_own, 0)

        flow(True, n - lag * z)
        flow(False, n - lag * (nz - 1 - z))

        @pl.when(n == close_at)
        def _():
            close_query()

        return carry

    lax.fori_loop(0, max(total + lag * (nz - 1), close_at + 1), step, 0)

    def close_rest(j, carry):
        slot = z * units + ny + j
        acc = with_sides(term(me, wrest[j]), z, j)
        at = pl.ds(pl.multiple_of(j * width, width), width)

        @pl.when(z == 0)
        def _():
            arrived(above.at[slot], above_got.at[slot])
            rest_out[:, at] = acc + above[slot].astype(F32)

        @pl.when(z == nz - 1)
        def _():
            arrived(below.at[slot], below_got.at[slot])
            rest_out[:, at] = acc + below[slot].astype(F32)

        @pl.when(jnp.logical_and(z > 0, z < nz - 1))
        def _():
            arrived(below.at[slot], below_got.at[slot])
            arrived(above.at[slot], above_got.at[slot])
            rest_out[:, at] = acc + below[slot].astype(F32) + above[slot].astype(F32)

        return carry

    lax.fori_loop(0, chunks, close_rest, 0)
    small = flat_out[me]
    for d in range(1, ny):
        arrived(last_in.at[d - 1], last_got.at[d - 1])
        q_out[...] = q_out[...] + last_in[d - 1].astype(F32)
        arrived(flat_last_in.at[d - 1], flast_got.at[d - 1])
        small = small + flat_last_in[d - 1]
    spare = jnp.zeros((LANES - small.shape[0], rows), F32)
    gates_out[...] = jnp.concatenate([small, spare], axis=0).T

    for d in range(1, ny):
        last(d).wait_send()
        flat_last(d).wait_send()

    def drain_side(u, carry):
        for d in range(1, ny):
            side(d, u // chunks, u % chunks).wait_send()
        return carry

    lax.fori_loop(0, nz * chunks, drain_side, 0)

    def drain_line(slot, carry):
        p = slot // units

        @pl.when(p > z)
        def _():
            line(True, slot).wait_send()

        @pl.when(p < z)
        def _():
            line(False, slot).wait_send()

        return carry

    lax.fori_loop(0, nz * units, drain_line, 0)

    def drain_flat(b, carry):
        @pl.when(b // ny > z)
        def _():
            flat_line(True, b).wait_send()

        @pl.when(b // ny < z)
        def _():
            flat_line(False, b).wait_send()

        return carry

    lax.fori_loop(0, nz * ny, drain_flat, 0)


def gather_sums(tokens, gain, gate_rows, query, key, value, outgate, ny, nz):
    kv = ny * nz
    depth = tokens.shape[1]
    rows = tokens.shape[0] // kv
    width = query.shape[1]
    chunks = (key.shape[1] + value.shape[1] + outgate.shape[1]) // width
    units = ny + chunks
    small = gate_rows.shape[0] + 8
    others = max(ny - 1, 1)
    vmem = pl.BlockSpec(memory_space=pltpu.VMEM)
    anywhere = pl.BlockSpec(memory_space=pl.ANY)
    dma = pltpu.SemaphoreType.DMA
    unit = (rows, width)
    tiny = (small, rows)
    return pl.pallas_call(
        functools.partial(gather_sums_kernel, ny, nz, 2),
        out_shape=[
            jax.ShapeDtypeStruct(unit, F32),
            jax.ShapeDtypeStruct((rows, chunks * width), F32),
            jax.ShapeDtypeStruct((rows, LANES), F32),
        ],
        in_specs=[anywhere, vmem, vmem] + [anywhere] * 4,
        out_specs=[vmem] * 3,
        scratch_shapes=[
            pltpu.VMEM(tokens.shape, BF16),
            pltpu.VMEM(tokens.shape, BF16),
            pltpu.VMEM((depth, width), BF16),
            pltpu.VMEM((chunks, depth, width), BF16),
            pltpu.VMEM((kv,) + tiny, F32),
            pltpu.VMEM((others, nz * chunks) + unit, BF16),
            pltpu.VMEM((others, nz * chunks) + unit, BF16),
            pltpu.VMEM((nz * units,) + unit, BF16),
            pltpu.VMEM((nz * units,) + unit, BF16),
            pltpu.VMEM((nz * units,) + unit, BF16),
            pltpu.VMEM((others,) + unit, BF16),
            pltpu.VMEM((others,) + unit, BF16),
            pltpu.VMEM((kv,) + tiny, F32),
            pltpu.VMEM((kv,) + tiny, F32),
            pltpu.VMEM((kv,) + tiny, F32),
            pltpu.VMEM((others,) + tiny, F32),
            pltpu.VMEM((others,) + tiny, F32),
            dma((2 + chunks,)),
            dma((others, nz * chunks)),
            dma((others, nz * chunks)),
            dma((nz * units,)),
            dma((nz * units,)),
            dma((nz * units,)),
            dma((others,)),
            dma((others,)),
            dma((kv,)),
            dma((kv,)),
            dma((kv,)),
            dma((others,)),
            dma((others,)),
        ],
        compiler_params=pltpu.CompilerParams(collective_id=1, has_side_effects=True),
        cost_estimate=pl.CostEstimate(
            flops=2 * kv * rows * depth * width * (chunks + 1),
            bytes_accessed=2 * depth * width * (chunks + 1),
            transcendentals=0,
        ),
        name="gather_sums",
    )(tokens, gain, gate_rows, query, key, value, outgate)


def per_device(
    kv,
    tp,
    tokens,
    norm_gain,
    query_weight,
    key_weight,
    value_weight,
    outgate_weight,
    gate_weight,
    forget_bias,
    head_gain,
    output_weight,
    state_matrix,
    state_normal,
    state_stable,
    prior_keys,
    prior_values,
    prior_ingate,
    prior_forget,
    accepted,
    parents,
):
    ny = 1 << ((kv.bit_length() - 1) // 2)
    nz = kv // ny
    me = lax.axis_index("kv")
    mine = lax.axis_index("tp")
    z, y = me // ny, lax.rem(me, ny)
    heads = query_weight.shape[1] // DQK
    depth = tokens.shape[1]
    seqs = accepted.shape[0]
    rows = seqs * PROP

    own_gain = lax.dynamic_slice_in_dim(norm_gain, me * depth, depth, 0)[None, :]
    head_start = mine * heads
    picked = lax.dynamic_slice_in_dim(
        gate_weight.reshape(depth, 2, HEADS), head_start, heads, 2
    ).reshape(depth, 2 * heads)
    sq_lane = -(-2 * heads // 8) * 8
    gate_rows = jnp.pad(picked.T, ((0, sq_lane - 2 * heads), (0, 0)))
    query, rest, gates = gather_sums(
        tokens, own_gain, gate_rows, query_weight, key_weight, value_weight, outgate_weight, ny, nz
    )

    live = (jnp.arange(PROP, dtype=jnp.int32)[None, :] < accepted[:, None])[:, :, None]
    forget_live = jnp.where(live, prior_forget, 0.0)
    cumul = [forget_live[:, 0]]
    for p in range(1, PROP):
        cumul.append(cumul[-1] + forget_live[:, p])
    total = cumul[-1]
    cumul = jnp.stack(cumul, axis=1)
    weight_log = jnp.where(live, total[:, None, :] - cumul + prior_ingate, -jnp.inf)
    new_stable = jnp.maximum(total + state_stable, jnp.max(weight_log, axis=1))
    weights = jnp.exp(weight_log - new_stable[:, None, :])
    decay = jnp.exp(total + state_stable - new_stable)
    new_normal = decay[:, :, None] * state_normal + jnp.sum(
        weights[..., None] * prior_keys.astype(F32).reshape(seqs, PROP, heads, DQK), axis=1
    )
    weight_rows = jnp.pad(weights.reshape(rows, heads), ((0, 0), (0, LANES - heads)))
    new_matrix, low_matrix = commit_matrix(
        decay,
        state_matrix,
        prior_keys.reshape(rows, heads * DQK),
        prior_values.reshape(rows, heads * DV),
        weight_rows,
        4,
    )

    step_rows = 32
    group = step_rows // PROP
    table = ancestry(parents)
    spread = (
        table.reshape(seqs // group, group, PROP, 1, PROP)
        * jnp.eye(group, dtype=F32)[None, :, None, :, None]
    ).reshape(rows, step_rows)
    stable_rows = jnp.pad(
        jnp.repeat(new_stable, PROP, axis=0), ((0, 0), (heads, LANES - 2 * heads))
    )
    normal_rows = jnp.repeat(new_normal.reshape(seqs, heads * DQK), PROP, axis=0)
    bias = jnp.pad(
        lax.dynamic_slice_in_dim(forget_bias, head_start, heads, 0), (heads, LANES - 2 * heads)
    )[None, :]

    hidden = tree_read(
        query,
        rest,
        gates,
        sq_lane,
        low_matrix,
        spread,
        stable_rows,
        normal_rows,
        bias,
        head_gain[None, :],
        step_rows,
    )

    layer_out = spread_out(hidden, output_weight, ny, nz, tp)
    return (layer_out, new_matrix, new_normal, new_stable)


def solution(mesh):
    placed = (
        P(None, "kv"),
        P(),
        P("kv", "tp"),
        P("kv", "tp"),
        P("kv", "tp"),
        P("kv", "tp"),
        P("kv", None),
        P(),
        P("tp"),
        P("tp", "kv"),
        P("kv", "tp", None, None),
        P("kv", "tp", None),
        P("kv", "tp"),
        P("kv", None, "tp"),
        P("kv", None, "tp"),
        P("kv", None, "tp"),
        P("kv", None, "tp"),
        P("kv"),
        P("kv", None),
    )
    return jax.shard_map(
        functools.partial(per_device, mesh.shape["kv"], mesh.shape["tp"]),
        mesh=mesh,
        in_specs=placed,
        out_specs=(P("tp", "kv"), P("kv", "tp", None, None), P("kv", "tp", None), P("kv", "tp")),
        check_vma=False,
    )
```

```python
import functools

import jax
import jax.numpy as jnp
from jax import lax
from jax.experimental import pallas as pl
from jax.experimental.pallas import tpu as pltpu
from jax.sharding import PartitionSpec as P

D = 4096
HEADS = 16
DQK = 128
DV = 256
PROP = 4
LANES = 128
NEG = -1e30
F32 = jnp.float32
BF16 = jnp.bfloat16
HP = lax.Precision.HIGHEST


def tree_kernel(
    q_ref, rest_ref, gates_ref, state_ref, mat, normal_ref, stable_ref, parent_ref, bias_ref,
    gain_ref, out_ref, mat_hbm, normal_out, stable_out, sem,
):
    mine = lax.axis_index("tp")
    rows = q_ref.shape[0]
    seqs, heads = mat.shape[:2]
    sq_lane = -(-2 * heads // 8) * 8
    stores = [pltpu.make_async_copy(mat.at[s], mat_hbm.at[s], sem.at[s]) for s in range(seqs)]
    for store in stores:
        store.start()
    stable_out[...] = stable_ref[...]

    def exact(a, b):
        return jnp.dot(a, b, precision=HP, preferred_element_type=F32)

    def iota(shape, axis):
        return lax.broadcasted_iota(jnp.int32, shape, axis)

    parents = parent_ref[...]
    current = iota((PROP, seqs), 0)
    tables = [(current == a).astype(F32) for a in range(PROP)]
    for repeat in range(PROP - 1):
        looked = jnp.zeros_like(current)
        for a in range(PROP):
            looked = looked + jnp.where(current == a, parents[a : a + 1], 0)
        current = jnp.where(current >= 0, looked, -1)
        tables = [t + (current == a).astype(F32) for a, t in enumerate(tables)]
    seq, at = iota((seqs, rows), 0), iota((seqs, rows), 1)
    packed = None
    for a, t in enumerate(tables):
        got = jnp.dot(
            t.astype(BF16), (at == seq * PROP + a).astype(F32).astype(BF16),
            preferred_element_type=F32,
        )
        packed = got if packed is None else packed + got
    spread = jnp.dot(
        (iota((rows, PROP), 0) % PROP == iota((rows, PROP), 1)).astype(F32).astype(BF16),
        packed.astype(BF16),
        preferred_element_type=F32,
    )
    same = iota((rows, rows), 0) // PROP == iota((rows, rows), 1) // PROP
    table = jnp.where(same, spread, 0.0)
    own = (iota((rows, seqs), 0) // PROP == iota((rows, seqs), 1)).astype(F32)

    gates = gates_ref[...]
    scale = lax.rsqrt(gates[:, sq_lane : sq_lane + 1] * (1.0 / D) + 1e-06)
    gates = scale * gates
    from_bias = (
        iota((HEADS, LANES), 0) + heads == iota((HEADS, LANES), 1) + mine * heads
    ).astype(F32)
    x = gates + exact(bias_ref[...], from_bias)
    logforget = jnp.minimum(x, 0.0) - jnp.log1p(jnp.exp(-jnp.abs(x)))
    path = exact(table, logforget)
    lifted = pltpu.roll(gates, heads, 1) - path
    flat = lifted.T
    stable = jnp.concatenate(
        [stable_ref[...], jnp.zeros((LANES - heads, seqs), F32)], axis=0
    )
    carried_all = path + pltpu.roll(
        lax.dot_general(
            own, stable, (((1,), (1,)), ((), ())), precision=HP, preferred_element_type=F32
        ),
        heads, 1,
    )
    key_scale = scale / jnp.sqrt(jnp.float32(DQK))
    at_value = heads * DQK
    at_gate = at_value + heads * DV
    for h in range(heads):
        normal = normal_ref[h]
        normal_out[:, h, :] = normal
        query = scale * q_ref[:, h * DQK : (h + 1) * DQK]
        value = scale * rest_ref[:, at_value + h * DV : at_value + (h + 1) * DV]
        key = key_scale * rest_ref[:, h * DQK : (h + 1) * DQK]
        outgate = scale * rest_ref[:, at_gate + h * DV : at_gate + (h + 1) * DV]
        dlog = path[:, heads + h : heads + h + 1] + flat[heads + h : heads + h + 1, :]
        dlog = jnp.where(table > 0.5, dlog, NEG)
        carried = carried_all[:, heads + h : heads + h + 1]
        top = jnp.maximum(carried, jnp.max(dlog, axis=1, keepdims=True))
        scores = lax.dot_general(
            query, key, (((1,), (1,)), ((), ())), precision=HP, preferred_element_type=F32
        ) * jnp.exp(dlog - top)
        factor = jnp.exp(carried - top)
        from_state = scale * state_ref[:, h * DV : (h + 1) * DV]
        numer = exact(scores, value) + factor * from_state
        denom = jnp.sum(scores, axis=1, keepdims=True) + factor * jnp.sum(
            query * exact(own, normal), axis=1, keepdims=True
        )
        read = numer / jnp.maximum(jnp.abs(denom), jnp.exp(-top))
        normer = lax.rsqrt(jnp.mean(read * read, axis=1, keepdims=True) + 1e-06)
        hidden = (
            read
            * normer
            * gain_ref[:, h * DV : (h + 1) * DV]
            * (1.0 / (1.0 + jnp.exp(-outgate)))
        )
        out_ref[:, h * DV : (h + 1) * DV] = hidden.astype(BF16)
    for store in stores:
        store.wait()


def tree_read(query, rest, gates, state, matrix, normal, stable, parents, bias, gain):
    rows = query.shape[0]
    seqs, heads = matrix.shape[:2]
    vmem = pl.BlockSpec(memory_space=pltpu.VMEM)
    return pl.pallas_call(
        tree_kernel,
        out_shape=[
            pltpu.VMEM((rows, heads * DV), BF16),
            jax.ShapeDtypeStruct(matrix.shape, F32),
            jax.ShapeDtypeStruct((seqs, heads, DQK), F32),
            jax.ShapeDtypeStruct((heads, seqs), F32),
        ],
        in_specs=[vmem] * 10,
        out_specs=[vmem, pl.BlockSpec(memory_space=pl.ANY), vmem, vmem],
        scratch_shapes=[pltpu.SemaphoreType.DMA((seqs,))],
        compiler_params=pltpu.CompilerParams(vmem_limit_bytes=16 << 20),
        cost_estimate=pl.CostEstimate(
            flops=8 * matrix.size, bytes_accessed=matrix.size * 4, transcendentals=0
        ),
        name="tree_read",
    )(query, rest, gates, state, matrix, normal, stable, parents, bias, gain)


def two_terms(full):
    lead = full.astype(BF16)
    return lead, (full - lead.astype(F32)).astype(BF16)


def fold(full, fine):
    return (full * full * full * jnp.abs(full) if fine else full).astype(BF16)


def unfold(sent, fine):
    full = sent.astype(F32)
    if not fine:
        return full
    root = jnp.sqrt(jnp.sqrt(jnp.abs(full)))
    return jnp.where(full < 0.0, -root, root)


def by_kind(j, act):
    if isinstance(j, int):
        act(j == 0)
    else:
        pl.when(j == 0)(lambda: act(True))
        pl.when(j > 0)(lambda: act(False))


def remote(src, dst, send_sem, recv_sem, kv_index, tp_index):
    return pltpu.make_async_remote_copy(
        src_ref=src,
        dst_ref=dst,
        send_sem=send_sem,
        recv_sem=recv_sem,
        device_id=(kv_index, tp_index),
        device_id_type=pl.DeviceIdType.MESH,
    )


def greet(others):
    barrier = pltpu.get_barrier_semaphore()
    for other in others:
        pl.semaphore_signal(
            barrier, inc=1, device_id=other, device_id_type=pl.DeviceIdType.MESH
        )
    pl.semaphore_wait(barrier, len(others))


def spread_kernel(
    ny, nz, tp, cuts, hid_ref, w_ref, out_ref, held, parts, landed, total,
    up_sem, down_sem, side_sem, got_sem, part_sem, land_sem,
):
    me = lax.axis_index("kv")
    mine = lax.axis_index("tp")
    z, y = me // ny, lax.rem(me, ny)
    kv = ny * nz
    per = kv // tp
    rows = hid_ref.shape[0]
    piece = rows // cuts
    greet(
        [((z + d) % nz * ny + y, mine) for d in sorted({1 % nz, nz - 1}) if d]
        + [(z * ny + (y + d) % ny, mine) for d in range(1, ny)]
        + [(me, (mine + d) % tp) for d in range(1, tp)]
    )

    def slab(b, c):
        return held.at[b, pl.ds(c * piece, piece)]

    def source(s, b, c):
        return hid_ref.at[pl.ds(c * piece, piece)] if s == 0 else slab(b, c)

    def up(s, b, c):
        return remote(source(s, b, c), slab(b, c), up_sem.at[s, c], got_sem.at[b, c], me + ny, mine)

    def down(s, b, c):
        return remote(source(s, b, c), slab(b, c), down_sem.at[s, c], got_sem.at[b, c], me - ny, mine)

    def side(s, b, c, d, way):
        return remote(
            source(s, b, c), slab(b, c), side_sem.at[way, s, d - 1, c], got_sem.at[b, c],
            z * ny + (y + d) % ny, mine,
        )

    def arrive(b, c):
        return remote(slab(b, c), slab(b, c), part_sem.at[b], got_sem.at[b, c], me, mine)

    def product(s, b):
        value = hid_ref[...] if s == 0 else held[b]
        got = jnp.dot(value, w_ref[...], preferred_element_type=F32)
        owner = b // per
        slot = b % per

        @pl.when(owner == mine)
        def _():
            total[slot] = got

        @pl.when(owner != mine)
        def _():
            parts[b] = got.astype(BF16)

    pending = []

    def hand_on():
        for there, b in pending:
            @pl.when(jnp.logical_and(there, b // per != mine))
            def _():
                hand(b).start()
        pending.clear()

    def hand(b):
        owner = b // per
        slot = ((mine + tp - owner) % tp + tp - 1) % tp * per + b % per
        return remote(parts.at[b], landed.at[slot], part_sem.at[b], land_sem.at[slot], me, owner)

    for c in range(cuts):
        @pl.when(z < nz - 1)
        def _():
            up(0, me, c).start()

        @pl.when(z > 0)
        def _():
            down(0, me, c).start()

        for d in range(1, ny):
            side(0, me, c, d, 0).start()
    product(0, me)
    pending.append((z >= 0, me))

    def from_side(s, way, there):
        base = (z - s + nz) % nz * ny if way == 0 else (z + s) % nz * ny
        for d in range(1, ny):
            b = base + (y + d) % ny

            @pl.when(there)
            def _():
                for c in range(cuts):
                    arrive(b, c).wait_recv()
                product(1, b)

            hand_on()
            pending.append((there, b))

    def ways(s):
        return [(0, z - s >= 0)] if s == 0 else [(0, z - s >= 0), (1, z + s < nz)]

    for s in range(1, nz):
        for way, there in ways(s):
            b = ((z - s + nz) % nz if way == 0 else (z + s) % nz) * ny + y

            @pl.when(there)
            def _():
                for c in range(cuts):
                    arrive(b, c).wait_recv()
                    if s < nz - 1:
                        if way == 0:
                            @pl.when(z < nz - 1)
                            def _():
                                up(s, b, c).start()
                        else:
                            @pl.when(z > 0)
                            def _():
                                down(s, b, c).start()
                    for d in range(1, ny):
                        side(s, b, c, d, way).start()
                product(s, b)

            hand_on()
            pending.append((there, b))

        for way, there in ways(s - 1):
            from_side(s - 1, way, there)

    for way, there in ways(nz - 1):
        from_side(nz - 1, way, there)
    hand_on()

    for slot in range(per):
        acc = total[slot]
        for d in range(1, tp):
            at = (d - 1) * per + slot
            remote(landed.at[at], landed.at[at], part_sem.at[0], land_sem.at[at], me, mine).wait_recv()
            acc = acc + landed[at].astype(F32)
        out_ref[slot * rows : (slot + 1) * rows] = acc.astype(BF16)

    for s in range(nz):
        for way, there in ways(s):
            b = ((z - s + nz) % nz if way == 0 else (z + s) % nz) * ny + y

            @pl.when(there)
            def _():
                for c in range(cuts):
                    if s < nz - 1:
                        if way == 0:
                            @pl.when(z < nz - 1)
                            def _():
                                up(s, b, c).wait_send()
                        if way == 1 or s == 0:
                            @pl.when(z > 0)
                            def _():
                                down(s, b, c).wait_send()
                    for d in range(1, ny):
                        side(s, b, c, d, way).wait_send()
    for b in range(kv):
        @pl.when(b // per != mine)
        def _():
            hand(b).wait_send()


def spread_out(hidden, weight, ny, nz, tp):
    rows, width = hidden.shape
    cols = weight.shape[1]
    kv = ny * nz
    per = kv // tp
    cuts = 2
    vmem = pl.BlockSpec(memory_space=pltpu.VMEM)
    dma = pltpu.SemaphoreType.DMA
    return pl.pallas_call(
        functools.partial(spread_kernel, ny, nz, tp, cuts),
        out_shape=jax.ShapeDtypeStruct((per * rows, cols), BF16),
        in_specs=[vmem, vmem],
        out_specs=vmem,
        scratch_shapes=[
            pltpu.VMEM((kv, rows, width), BF16),
            pltpu.VMEM((kv, rows, cols), BF16),
            pltpu.VMEM(((tp - 1) * per, rows, cols), BF16),
            pltpu.VMEM((per, rows, cols), F32),
            dma((nz, cuts)),
            dma((nz, cuts)),
            dma((2, nz, max(ny - 1, 1), cuts)),
            dma((kv, cuts)),
            dma((kv,)),
            dma(((tp - 1) * per,)),
        ],
        compiler_params=pltpu.CompilerParams(
            collective_id=0, has_side_effects=True, vmem_limit_bytes=16 << 20
        ),
        cost_estimate=pl.CostEstimate(
            flops=2 * kv * rows * width * cols, bytes_accessed=8 * rows * width, transcendentals=0
        ),
        name="spread",
    )(hidden, weight)


def gather_sums_kernel(
    ny, nz, lag, tok_hbm, gain_ref, gate_ref, q_hbm, k_hbm, v_hbm, o_hbm, state_hbm,
    pk_ref, pv_ref, pin_ref, pfo_ref, stable_ref, count_ref, normal_ref,
    q_out, rest_out, gates_out, state_out, mat, normal_out, stable_out,
    tok, normed, wq, wrest, flat,
    side_out, side_in, line_out, below, above, last_out, last_in,
    flat_out, flat_below, flat_above, flat_last_out, flat_last_in,
    wide, kt, vw, decay, work,
    load_sem, side_sem, side_got, line_sem, below_got, above_got, last_sem, last_got,
    fline_sem, fbelow_got, fabove_got, flast_sem, flast_got, state_sem,
):
    me = lax.axis_index("kv")
    mine = lax.axis_index("tp")
    z, y = me // ny, lax.rem(me, ny)
    rows = q_out.shape[0]
    width = wq.shape[1]
    chunks = wrest.shape[0]
    units = ny + chunks
    seqs, heads = mat.shape[:2]
    depth = tok.shape[1]

    loads = [
        pltpu.make_async_copy(tok_hbm, tok, load_sem.at[0]),
        pltpu.make_async_copy(q_hbm, wq, load_sem.at[1]),
    ]
    for n, (w, at) in enumerate(
        [(w, at) for w in (k_hbm, v_hbm, o_hbm) for at in range(0, w.shape[1], width)]
    ):
        loads.append(
            pltpu.make_async_copy(w.at[:, pl.ds(at, width)], wrest.at[n], load_sem.at[2 + n])
        )
    for load in loads:
        load.start()

    def state_load(s):
        return pltpu.make_async_copy(state_hbm.at[s], mat.at[s], state_sem.at[s])

    greet(
        [((z + d) % nz * ny + y, mine) for d in sorted({1 % nz, nz - 1}) if d]
        + [(z * ny + (y + d) % ny, mine) for d in range(1, ny)]
    )
    loads[0].wait()
    gain = gain_ref[:, pl.ds(pl.multiple_of(me * depth, LANES), depth)]

    def prepare(n, carry):
        at = pl.ds(pl.multiple_of(n * rows, rows), rows)
        normed[at, :] = (tok[at, :].astype(F32) * gain).astype(BF16)
        return carry

    lax.fori_loop(0, ny * nz, prepare, 0)
    for load in loads[1:]:
        load.wait()

    small = flat.shape[1] - 8
    row = lax.broadcasted_iota(jnp.int32, (small, 2 * HEADS), 0)
    col = lax.broadcasted_iota(jnp.int32, (small, 2 * HEADS), 1)
    want = jnp.where(row < heads, row, HEADS - heads + row) + mine * heads
    picked = jnp.where(jnp.logical_and(row < 2 * heads, col == want), 1.0, 0.0).astype(BF16)
    gate_rows = jnp.dot(picked, gate_ref[...], preferred_element_type=F32).astype(BF16)

    def flats(n, carry):
        at = pl.ds(pl.multiple_of(n * rows, rows), rows)
        x = tok[at, :].astype(F32)
        full = x * x
        lead = full.astype(BF16)
        rest = (full - lead.astype(F32)).astype(BF16)
        ones = jnp.ones((8, depth), BF16)

        def across(a, b):
            return lax.dot_general(a, b, (((1,), (1,)), ((), ())), preferred_element_type=F32)

        flat[n] = jnp.concatenate(
            [across(gate_rows, normed[at, :]), across(ones, lead) + across(ones, rest)], axis=0
        )
        return carry

    def term(block, w):
        at = pl.ds(pl.multiple_of(block * rows, rows), rows)
        return jnp.dot(normed[at, :], w, preferred_element_type=F32)

    def side(d, p, j):
        u = p * chunks + j
        return remote(
            side_out.at[d - 1, u], side_in.at[ny - d - 1, u], side_sem.at[d - 1, u],
            side_got.at[ny - d - 1, u], z * ny + (y + d) % ny, mine,
        )

    def line(going_up, slot):
        got, sem, far = (below, below_got, me + ny) if going_up else (above, above_got, me - ny)
        return remote(line_out.at[slot], got.at[slot], line_sem.at[slot], sem.at[slot], far, mine)

    def flat_line(going_up, b):
        got, sem, far = (
            (flat_below, fbelow_got, me + ny) if going_up else (flat_above, fabove_got, me - ny)
        )
        return remote(flat_out.at[b], got.at[b], fline_sem.at[b], sem.at[b], far, mine)

    def last(d):
        return remote(
            last_out.at[d - 1], last_in.at[ny - d - 1], last_sem.at[d - 1],
            last_got.at[ny - d - 1], z * ny + (y + d) % ny, mine,
        )

    def flat_last(d):
        return remote(
            flat_last_out.at[d - 1], flat_last_in.at[ny - d - 1], flast_sem.at[d - 1],
            flast_got.at[ny - d - 1], z * ny + (y + d) % ny, mine,
        )

    def arrived(ref, sem):
        remote(ref, ref, load_sem.at[0], sem, me, mine).wait_recv()

    def fill_side(p, j):
        for d in range(1, ny):
            work[...] = term(p * ny + (y + d) % ny, wrest[j])

            def put(fine):
                side_out[d - 1, p * chunks + j] = fold(work[...], fine)

            by_kind(j, put)

    def start_side(p, j):
        for d in range(1, ny):
            side(d, p, j).start()

    def each_side(n, act):
        i, j = n // chunks, n % chunks

        @pl.when(jnp.logical_and(i < nz - 1, nz - 1 - i > z))
        def _():
            act(nz - 1 - i, j)

        @pl.when(i < z)
        def _():
            act(i, j)

        @pl.when(i == nz - 1)
        def _():
            act(z, j)

    def side_round(n, carry):
        each_side(n, fill_side)

        @pl.when(n > 0)
        def _():
            each_side(n - 1, start_side)

        return carry

    def add(ref, at, sem, j):
        arrived(ref.at[at], sem.at[at])

        def more(fine):
            work[...] = work[...] + unfold(ref[at], fine)

        by_kind(j, more)

    def add_sides(p, j):
        for d in range(1, ny):
            add(side_in, (d - 1, p * chunks + j), side_got, j)

    def pass_on(going_up, slot, j):
        got, sem = (below, below_got) if going_up else (above, above_got)

        @pl.when(z > 0 if going_up else z < nz - 1)
        def _():
            add(got, slot, sem, j)

        def put(fine):
            line_out[slot] = fold(work[...], fine)

        by_kind(j, put)

    def pass_flat(going_up, b):
        got, sem = (flat_below, fbelow_got) if going_up else (flat_above, fabove_got)
        first = z == 0 if going_up else z == nz - 1

        @pl.when(first)
        def _():
            flat_out[b] = flat[b]

        @pl.when(jnp.logical_not(first))
        def _():
            arrived(got.at[b], sem.at[b])
            flat_out[b] = flat[b] + got[b]

    early = (nz - 1) * ny
    total = early + (nz - 1) * chunks

    def plane_of(going_up, i):
        return nz - 1 - i if going_up else i

    def flow(going_up, n, send):
        @pl.when(jnp.logical_and(n >= 0, n < early))
        def _():
            p = plane_of(going_up, n // ny)

            @pl.when(p > z if going_up else p < z)
            def _():
                b = p * ny + n % ny
                if send:
                    flat_line(going_up, b).start()
                    line(going_up, p * units + n % ny).start()
                else:
                    pass_flat(going_up, b)
                    work[...] = term(b, wq[...])
                    pass_on(going_up, p * units + n % ny, 0)

        @pl.when(jnp.logical_and(n >= early, n < total))
        def _():
            p = plane_of(going_up, (n - early) // chunks)
            j = (n - early) % chunks

            @pl.when(p > z if going_up else p < z)
            def _():
                slot = p * units + ny + j
                if send:
                    line(going_up, slot).start()
                else:
                    work[...] = term(p * ny + y, wrest[j])
                    add_sides(p, j)
                    pass_on(going_up, slot, j)

    def close_query():
        for d in range(ny):
            yy = (y + d) % ny
            b, slot = z * ny + yy, z * units + yy
            acc = term(b, wq[...])
            small = flat[b]

            def keep(acc, small):
                if d == 0:
                    q_out[...] = acc
                    flat_out[b] = small
                else:
                    last_out[d - 1] = fold(acc, True)
                    flat_last_out[d - 1] = small

            def lower():
                arrived(below.at[slot], below_got.at[slot])
                arrived(flat_below.at[b], fbelow_got.at[b])
                return unfold(below[slot], True), flat_below[b]

            def upper():
                arrived(above.at[slot], above_got.at[slot])
                arrived(flat_above.at[b], fabove_got.at[b])
                return unfold(above[slot], True), flat_above[b]

            @pl.when(z == 0)
            def _():
                more, less = upper()
                keep(acc + more, small + less)

            @pl.when(z == nz - 1)
            def _():
                more, less = lower()
                keep(acc + more, small + less)

            @pl.when(jnp.logical_and(z > 0, z < nz - 1))
            def _():
                more, less = lower()
                again, still = upper()
                keep(acc + more + again, small + less + still)


    def exact(a, b):
        return jnp.dot(a, b, precision=HP, preferred_element_type=F32)

    def prepare_commit():
        run = None
        sums, lives = [], []
        for p in range(PROP):
            live = count_ref[...] > p
            here = jnp.where(live, pfo_ref[p], 0.0)
            run = here if run is None else run + here
            sums.append(run)
            lives.append(live)
        logs = [
            jnp.where(live, run - part + pin_ref[p], NEG)
            for p, (live, part) in enumerate(zip(lives, sums))
        ]
        carried = run + stable_ref[...]
        top = carried
        for log in logs:
            top = jnp.maximum(top, log)
        stable_out[...] = top
        seq = lax.broadcasted_iota(jnp.int32, (seqs, rows), 0)
        at = lax.broadcasted_iota(jnp.int32, (seqs, rows), 1)
        flat_weights = None
        for p, log in enumerate(logs):
            got = exact(jnp.exp(log - top), (at == seq * PROP + p).astype(F32))
            flat_weights = got if flat_weights is None else flat_weights + got
        spare = jnp.zeros((LANES - heads, rows), F32)
        weights = jnp.concatenate([flat_weights, spare], axis=0).T
        lanes = (
            lax.broadcasted_iota(jnp.int32, (seqs, LANES), 0)
            == lax.broadcasted_iota(jnp.int32, (seqs, LANES), 1)
        ).astype(F32)
        flat_decay = jnp.concatenate(
            [exact(jnp.exp(carried - top), lanes), jnp.zeros((LANES - heads, LANES), F32)], axis=0
        ).T

        pair = 8 // PROP

        def gather_keys(i, carry):
            to = pl.ds(pl.multiple_of(i * 8, 8), 8)
            got = [pk_ref[i * pair + n].astype(F32) for n in range(pair)]
            wide[to, : heads * DQK] = jnp.concatenate(got, axis=0)
            return carry

        lax.fori_loop(0, seqs // pair, gather_keys, 0)
        for h in range(heads):
            keys = wide[:, h * DQK : (h + 1) * DQK]
            kt[h] = keys.T
            mine_only = jnp.where(at // PROP == seq, flat_weights[h : h + 1], 0.0)
            fade = jnp.broadcast_to(flat_decay[:seqs, h : h + 1], (seqs, DV))
            decay[h] = fade
            normal_out[h] = fade[:, :DQK] * normal_ref[:, h, :] + exact(mine_only, keys)

        def gather_values(i, carry):
            to = pl.ds(pl.multiple_of(i * 8, 8), 8)
            got = [pv_ref[i * pair + n].astype(F32) for n in range(pair)]
            wide[to, :] = jnp.concatenate(got, axis=0)
            return carry

        lax.fori_loop(0, seqs // pair, gather_values, 0)
        for h in range(heads):
            at_h = slice(h * DV, (h + 1) * DV)
            lead, rest = two_terms(wide[:, at_h] * weights[:, h : h + 1])
            vw[:rows, at_h] = lead
            vw[rows:, at_h] = rest

    def commit(s):
        state_load(s).wait()
        own = lax.broadcasted_iota(jnp.int32, (DQK, rows), 1) // PROP == s
        for h in range(heads):
            lhs = jnp.where(own, kt[h], 0.0).astype(BF16)
            lhs = jnp.concatenate([lhs, lhs], axis=1)
            added = jnp.dot(lhs, vw[:, h * DV : (h + 1) * DV], preferred_element_type=F32)
            mat[s, h] = decay[h, pl.ds(s, 1), :] * mat[s, h] + added

    def finish_query():
        for d in range(1, ny):
            arrived(last_in.at[d - 1], last_got.at[d - 1])
            q_out[...] = q_out[...] + unfold(last_in[d - 1], True)

    def state_product(g):
        at = pl.ds(pl.multiple_of(g * 16, 16), 16)
        row16 = lax.broadcasted_iota(jnp.int32, (16, 1), 0) // PROP
        for h in range(heads):
            part, less = two_terms(q_out[at, h * DQK : (h + 1) * DQK])
            both = jnp.concatenate([part, less], axis=0)
            got = None
            for n in range(16 // PROP):
                lead, rest = two_terms(mat[g * (16 // PROP) + n, h])
                res = jnp.dot(both, lead, preferred_element_type=F32)
                res = res[:16] + res[16:] + jnp.dot(part, rest, preferred_element_type=F32)
                got = res if got is None else jnp.where(row16 == n, res, got)
            state_out[at, h * DV : (h + 1) * DV] = got

    lax.fori_loop(0, chunks + 1, side_round, 0)
    lax.fori_loop(0, ny * nz, flats, 0)
    close_at = early + lag * (nz - 1) + 1
    groups = rows // 16
    product_at = max(close_at + 2, 2 + seqs // 2)

    def step(n, carry):
        up_at, down_at = n - lag * z, n - lag * (nz - 1 - z)
        flow(True, up_at, False)
        flow(False, down_at, False)

        @pl.when(n == close_at)
        def _():
            close_query()

        @pl.when(jnp.logical_and(n >= 2, n < 2 + seqs // 2))
        def _():
            commit(2 * (n - 2))

        @pl.when(n == product_at)
        def _():
            finish_query()

        flow(True, up_at, True)
        flow(False, down_at, True)

        @pl.when(n == close_at)
        def _():
            for d in range(1, ny):
                last(d).start()
                flat_last(d).start()

        @pl.when(n == 1)
        def _():
            lax.fori_loop(chunks + 1, nz * chunks, side_round, 0)
            each_side(nz * chunks - 1, start_side)
            for s in range(seqs):
                state_load(s).start()
            prepare_commit()

        @pl.when(jnp.logical_and(n >= 2, n < 2 + seqs // 2))
        def _():
            commit(2 * (n - 2) + 1)

        @pl.when(jnp.logical_and(n >= product_at, n < product_at + groups))
        def _():
            state_product(n - product_at)

        return carry

    lax.fori_loop(0, max(total + lag * (nz - 1), product_at + groups), step, 0)

    def close_rest(j, carry):
        slot = z * units + ny + j
        work[...] = term(me, wrest[j])
        add_sides(z, j)

        @pl.when(z > 0)
        def _():
            add(below, slot, below_got, j)

        @pl.when(z < nz - 1)
        def _():
            add(above, slot, above_got, j)

        at = pl.ds(pl.multiple_of(j * width, width), width)
        rest_out[:, at] = work[...]
        return carry

    lax.fori_loop(0, chunks, close_rest, 0)
    small = flat_out[me]
    for d in range(1, ny):
        arrived(flat_last_in.at[d - 1], flast_got.at[d - 1])
        small = small + flat_last_in[d - 1]
    spare = jnp.zeros((LANES - small.shape[0], rows), F32)
    gates_out[...] = jnp.concatenate([small, spare], axis=0).T

    for d in range(1, ny):
        last(d).wait_send()
        flat_last(d).wait_send()

    def drain_side(u, carry):
        for d in range(1, ny):
            side(d, u // chunks, u % chunks).wait_send()
        return carry

    lax.fori_loop(0, nz * chunks, drain_side, 0)

    def drain_line(slot, carry):
        p = slot // units

        @pl.when(p > z)
        def _():
            line(True, slot).wait_send()

        @pl.when(p < z)
        def _():
            line(False, slot).wait_send()

        return carry

    lax.fori_loop(0, nz * units, drain_line, 0)

    def drain_flat(b, carry):
        @pl.when(b // ny > z)
        def _():
            flat_line(True, b).wait_send()

        @pl.when(b // ny < z)
        def _():
            flat_line(False, b).wait_send()

        return carry

    lax.fori_loop(0, nz * ny, drain_flat, 0)


def gather_sums(
    tokens, gain, gates, query, key, value, outgate, state, prior_keys, prior_values,
    ingate, forget, stable, count, normal, ny, nz,
):
    kv = ny * nz
    depth = tokens.shape[1]
    rows = tokens.shape[0] // kv
    width = query.shape[1]
    chunks = (key.shape[1] + value.shape[1] + outgate.shape[1]) // width
    units = ny + chunks
    seqs, heads = state.shape[:2]
    small = -(-2 * heads // 8) * 8 + 8
    others = max(ny - 1, 1)
    vmem = pl.BlockSpec(memory_space=pltpu.VMEM)
    anywhere = pl.BlockSpec(memory_space=pl.ANY)
    dma = pltpu.SemaphoreType.DMA
    unit = (rows, width)
    tiny = (small, rows)
    return pl.pallas_call(
        functools.partial(gather_sums_kernel, ny, nz, 2),
        out_shape=[
            pltpu.VMEM(unit, F32),
            pltpu.VMEM((rows, chunks * width), F32),
            pltpu.VMEM((rows, LANES), F32),
            pltpu.VMEM((rows, heads * DV), F32),
            pltpu.VMEM(state.shape, F32),
            pltpu.VMEM((heads, seqs, DQK), F32),
            pltpu.VMEM((heads, seqs), F32),
        ],
        in_specs=[anywhere, vmem, vmem] + [anywhere] * 5 + [vmem] * 7,
        out_specs=[vmem] * 7,
        scratch_shapes=[
            pltpu.VMEM(tokens.shape, BF16),
            pltpu.VMEM(tokens.shape, BF16),
            pltpu.VMEM((depth, width), BF16),
            pltpu.VMEM((chunks, depth, width), BF16),
            pltpu.VMEM((kv,) + tiny, F32),
            pltpu.VMEM((others, nz * chunks) + unit, BF16),
            pltpu.VMEM((others, nz * chunks) + unit, BF16),
            pltpu.VMEM((nz * units,) + unit, BF16),
            pltpu.VMEM((nz * units,) + unit, BF16),
            pltpu.VMEM((nz * units,) + unit, BF16),
            pltpu.VMEM((others,) + unit, BF16),
            pltpu.VMEM((others,) + unit, BF16),
            pltpu.VMEM((kv,) + tiny, F32),
            pltpu.VMEM((kv,) + tiny, F32),
            pltpu.VMEM((kv,) + tiny, F32),
            pltpu.VMEM((others,) + tiny, F32),
            pltpu.VMEM((others,) + tiny, F32),
            pltpu.VMEM((rows, heads * DV), F32),
            pltpu.VMEM((heads, DQK, rows), F32),
            pltpu.VMEM((2 * rows, heads * DV), BF16),
            pltpu.VMEM((heads, seqs, DV), F32),
            pltpu.VMEM(unit, F32),
            dma((2 + chunks,)),
            dma((others, nz * chunks)),
            dma((others, nz * chunks)),
            dma((nz * units,)),
            dma((nz * units,)),
            dma((nz * units,)),
            dma((others,)),
            dma((others,)),
            dma((kv,)),
            dma((kv,)),
            dma((kv,)),
            dma((others,)),
            dma((others,)),
            dma((seqs,)),
        ],
        compiler_params=pltpu.CompilerParams(
            collective_id=1, has_side_effects=True, vmem_limit_bytes=36 << 20
        ),
        cost_estimate=pl.CostEstimate(
            flops=2 * kv * rows * depth * width * (chunks + 1),
            bytes_accessed=2 * depth * width * (chunks + 1) + 4 * state.size,
            transcendentals=0,
        ),
        name="gather_sums",
    )(
        tokens, gain, gates, query, key, value, outgate, state, prior_keys, prior_values,
        ingate, forget, stable, count, normal,
    )


def per_device(
    kv,
    tp,
    tokens,
    norm_gain,
    query_weight,
    key_weight,
    value_weight,
    outgate_weight,
    gate_weight,
    forget_bias,
    head_gain,
    output_weight,
    state_matrix,
    state_normal,
    state_stable,
    prior_keys,
    prior_values,
    prior_ingate,
    prior_forget,
    accepted,
    parents,
):
    ny = 1 << ((kv.bit_length() - 1) // 2)
    nz = kv // ny
    query, rest, gates, state, matrix, normal, stable = gather_sums(
        tokens,
        norm_gain[None, :],
        gate_weight.T,
        query_weight,
        key_weight,
        value_weight,
        outgate_weight,
        state_matrix,
        prior_keys,
        prior_values,
        prior_ingate.transpose(1, 2, 0),
        prior_forget.transpose(1, 2, 0),
        state_stable.T,
        accepted[None, :],
        state_normal,
        ny,
        nz,
    )
    hidden, new_matrix, new_normal, new_stable = tree_read(
        query,
        rest,
        gates,
        state,
        matrix,
        normal,
        stable,
        parents.T,
        forget_bias[None, :],
        head_gain[None, :],
    )
    layer_out = spread_out(hidden, output_weight, ny, nz, tp)
    return (layer_out, new_matrix, new_normal, new_stable.T)


def solution(mesh):
    placed = (
        P(None, "kv"),
        P(),
        P("kv", "tp"),
        P("kv", "tp"),
        P("kv", "tp"),
        P("kv", "tp"),
        P("kv", None),
        P(),
        P("tp"),
        P("tp", "kv"),
        P("kv", "tp", None, None),
        P("kv", "tp", None),
        P("kv", "tp"),
        P("kv", None, "tp"),
        P("kv", None, "tp"),
        P("kv", None, "tp"),
        P("kv", None, "tp"),
        P("kv"),
        P("kv", None),
    )
    return jax.shard_map(
        functools.partial(per_device, mesh.shape["kv"], mesh.shape["tp"]),
        mesh=mesh,
        in_specs=placed,
        out_specs=(P("tp", "kv"), P("kv", "tp", None, None), P("kv", "tp", None), P("kv", "tp")),
        check_vma=False,
    )
```

```python
import functools

import jax
import jax.numpy as jnp
from jax import lax
from jax.experimental import pallas as pl
from jax.experimental.pallas import tpu as pltpu
from jax.sharding import PartitionSpec as P

D = 4096
HEADS = 16
DQK = 128
DV = 256
PROP = 4
LANES = 128
NEG = -1e30
F32 = jnp.float32
BF16 = jnp.bfloat16
HP = lax.Precision.HIGHEST


def tree_kernel(
    q_ref, rest_ref, gates_ref, state_ref, mat, normal_ref, stable_ref, parent_ref, bias_ref,
    gain_ref, out_ref, mat_hbm, normal_out, stable_out, sem,
):
    mine = lax.axis_index("tp")
    rows = q_ref.shape[0]
    seqs, heads = mat.shape[:2]
    sq_lane = -(-2 * heads // 8) * 8
    stores = [pltpu.make_async_copy(mat.at[s], mat_hbm.at[s], sem.at[s]) for s in range(seqs)]
    for store in stores:
        store.start()
    stable_out[...] = stable_ref[...]

    def exact(a, b):
        return jnp.dot(a, b, precision=HP, preferred_element_type=F32)

    def iota(shape, axis):
        return lax.broadcasted_iota(jnp.int32, shape, axis)

    parents = parent_ref[...]
    current = iota((PROP, seqs), 0)
    tables = [(current == a).astype(F32) for a in range(PROP)]
    for repeat in range(PROP - 1):
        looked = jnp.zeros_like(current)
        for a in range(PROP):
            looked = looked + jnp.where(current == a, parents[a : a + 1], 0)
        current = jnp.where(current >= 0, looked, -1)
        tables = [t + (current == a).astype(F32) for a, t in enumerate(tables)]
    seq, at = iota((seqs, rows), 0), iota((seqs, rows), 1)
    packed = None
    for a, t in enumerate(tables):
        got = jnp.dot(
            t.astype(BF16), (at == seq * PROP + a).astype(F32).astype(BF16),
            preferred_element_type=F32,
        )
        packed = got if packed is None else packed + got
    spread = jnp.dot(
        (iota((rows, PROP), 0) % PROP == iota((rows, PROP), 1)).astype(F32).astype(BF16),
        packed.astype(BF16),
        preferred_element_type=F32,
    )
    same = iota((rows, rows), 0) // PROP == iota((rows, rows), 1) // PROP
    table = jnp.where(same, spread, 0.0)
    own = (iota((rows, seqs), 0) // PROP == iota((rows, seqs), 1)).astype(F32)

    gates = gates_ref[...]
    scale = lax.rsqrt(gates[:, sq_lane : sq_lane + 1] * (1.0 / D) + 1e-06)
    gates = scale * gates
    from_bias = (
        iota((HEADS, LANES), 0) + heads == iota((HEADS, LANES), 1) + mine * heads
    ).astype(F32)
    x = gates + exact(bias_ref[...], from_bias)
    logforget = jnp.minimum(x, 0.0) - jnp.log1p(jnp.exp(-jnp.abs(x)))
    path = exact(table, logforget)
    lifted = pltpu.roll(gates, heads, 1) - path
    flat = lifted.T
    stable = jnp.concatenate(
        [stable_ref[...], jnp.zeros((LANES - heads, seqs), F32)], axis=0
    )
    carried_all = path + pltpu.roll(
        lax.dot_general(
            own, stable, (((1,), (1,)), ((), ())), precision=HP, preferred_element_type=F32
        ),
        heads, 1,
    )
    key_scale = scale / jnp.sqrt(jnp.float32(DQK))
    at_value = heads * DQK
    at_gate = at_value + heads * DV
    for h in range(heads):
        normal = normal_ref[h]
        normal_out[:, h, :] = normal
        query = scale * q_ref[:, h * DQK : (h + 1) * DQK]
        value = scale * rest_ref[:, at_value + h * DV : at_value + (h + 1) * DV]
        key = key_scale * rest_ref[:, h * DQK : (h + 1) * DQK]
        outgate = scale * rest_ref[:, at_gate + h * DV : at_gate + (h + 1) * DV]
        dlog = path[:, heads + h : heads + h + 1] + flat[heads + h : heads + h + 1, :]
        dlog = jnp.where(table > 0.5, dlog, NEG)
        carried = carried_all[:, heads + h : heads + h + 1]
        top = jnp.maximum(carried, jnp.max(dlog, axis=1, keepdims=True))
        scores = lax.dot_general(
            query, key, (((1,), (1,)), ((), ())), precision=HP, preferred_element_type=F32
        ) * jnp.exp(dlog - top)
        factor = jnp.exp(carried - top)
        from_state = scale * state_ref[:, h * DV : (h + 1) * DV]
        numer = exact(scores, value) + factor * from_state
        denom = jnp.sum(scores, axis=1, keepdims=True) + factor * jnp.sum(
            query * exact(own, normal), axis=1, keepdims=True
        )
        read = numer / jnp.maximum(jnp.abs(denom), jnp.exp(-top))
        normer = lax.rsqrt(jnp.mean(read * read, axis=1, keepdims=True) + 1e-06)
        hidden = (
            read
            * normer
            * gain_ref[:, h * DV : (h + 1) * DV]
            * (1.0 / (1.0 + jnp.exp(-outgate)))
        )
        out_ref[:, h * DV : (h + 1) * DV] = hidden.astype(BF16)
    for store in stores:
        store.wait()


def tree_read(query, rest, gates, state, matrix, normal, stable, parents, bias, gain):
    rows = query.shape[0]
    seqs, heads = matrix.shape[:2]
    vmem = pl.BlockSpec(memory_space=pltpu.VMEM)
    return pl.pallas_call(
        tree_kernel,
        out_shape=[
            pltpu.VMEM((rows, heads * DV), BF16),
            jax.ShapeDtypeStruct(matrix.shape, F32),
            jax.ShapeDtypeStruct((seqs, heads, DQK), F32),
            jax.ShapeDtypeStruct((heads, seqs), F32),
        ],
        in_specs=[vmem] * 10,
        out_specs=[vmem, pl.BlockSpec(memory_space=pl.ANY), vmem, vmem],
        scratch_shapes=[pltpu.SemaphoreType.DMA((seqs,))],
        compiler_params=pltpu.CompilerParams(vmem_limit_bytes=16 << 20),
        cost_estimate=pl.CostEstimate(
            flops=8 * matrix.size, bytes_accessed=matrix.size * 4, transcendentals=0
        ),
        name="tree_read",
    )(query, rest, gates, state, matrix, normal, stable, parents, bias, gain)


def two_terms(full):
    lead = full.astype(BF16)
    return lead, (full - lead.astype(F32)).astype(BF16)


def fold(full, fine):
    return (full * full * full * jnp.abs(full) if fine else full).astype(BF16)


def unfold(sent, fine):
    full = sent.astype(F32)
    if not fine:
        return full
    root = jnp.sqrt(jnp.sqrt(jnp.abs(full)))
    return jnp.where(full < 0.0, -root, root)


def by_kind(j, act):
    if isinstance(j, int):
        act(j == 0)
    else:
        pl.when(j == 0)(lambda: act(True))
        pl.when(j > 0)(lambda: act(False))


def remote(src, dst, send_sem, recv_sem, kv_index, tp_index):
    return pltpu.make_async_remote_copy(
        src_ref=src,
        dst_ref=dst,
        send_sem=send_sem,
        recv_sem=recv_sem,
        device_id=(kv_index, tp_index),
        device_id_type=pl.DeviceIdType.MESH,
    )


def greet(others):
    barrier = pltpu.get_barrier_semaphore()
    for other in others:
        pl.semaphore_signal(
            barrier, inc=1, device_id=other, device_id_type=pl.DeviceIdType.MESH
        )
    pl.semaphore_wait(barrier, len(others))


def spread_kernel(
    ny, nz, tp, cuts, hid_ref, w_ref, out_ref, held, parts, landed, total,
    up_sem, down_sem, side_sem, got_sem, part_sem, land_sem,
):
    me = lax.axis_index("kv")
    mine = lax.axis_index("tp")
    z, y = me // ny, lax.rem(me, ny)
    kv = ny * nz
    per = kv // tp
    rows = hid_ref.shape[0]
    piece = rows // cuts
    greet(
        [((z + d) % nz * ny + y, mine) for d in sorted({1 % nz, nz - 1}) if d]
        + [(z * ny + (y + d) % ny, mine) for d in range(1, ny)]
        + [(me, (mine + d) % tp) for d in range(1, tp)]
    )

    def slab(b, c):
        return held.at[b, pl.ds(c * piece, piece)]

    def source(s, b, c):
        return hid_ref.at[pl.ds(c * piece, piece)] if s == 0 else slab(b, c)

    def up(s, b, c):
        return remote(source(s, b, c), slab(b, c), up_sem.at[s, c], got_sem.at[b, c], me + ny, mine)

    def down(s, b, c):
        return remote(source(s, b, c), slab(b, c), down_sem.at[s, c], got_sem.at[b, c], me - ny, mine)

    def side(s, b, c, d, way):
        return remote(
            source(s, b, c), slab(b, c), side_sem.at[way, s, d - 1, c], got_sem.at[b, c],
            z * ny + (y + d) % ny, mine,
        )

    def arrive(b, c):
        return remote(slab(b, c), slab(b, c), part_sem.at[b], got_sem.at[b, c], me, mine)

    def product(s, b):
        value = hid_ref[...] if s == 0 else held[b]
        got = jnp.dot(value, w_ref[...], preferred_element_type=F32)
        owner = b // per
        slot = b % per

        @pl.when(owner == mine)
        def _():
            total[slot] = got

        @pl.when(owner != mine)
        def _():
            parts[b] = got.astype(BF16)

    pending = []

    def hand_on():
        for there, b in pending:
            @pl.when(jnp.logical_and(there, b // per != mine))
            def _():
                hand(b).start()
        pending.clear()

    def hand(b):
        owner = b // per
        slot = ((mine + tp - owner) % tp + tp - 1) % tp * per + b % per
        return remote(parts.at[b], landed.at[slot], part_sem.at[b], land_sem.at[slot], me, owner)

    for c in range(cuts):
        @pl.when(z < nz - 1)
        def _():
            up(0, me, c).start()

        @pl.when(z > 0)
        def _():
            down(0, me, c).start()

        for d in range(1, ny):
            side(0, me, c, d, 0).start()
    product(0, me)
    pending.append((z >= 0, me))

    def from_side(s, way, there):
        base = (z - s + nz) % nz * ny if way == 0 else (z + s) % nz * ny
        for d in range(1, ny):
            b = base + (y + d) % ny

            @pl.when(there)
            def _():
                for c in range(cuts):
                    arrive(b, c).wait_recv()
                product(1, b)

            hand_on()
            pending.append((there, b))

    def ways(s):
        return [(0, z - s >= 0)] if s == 0 else [(0, z - s >= 0), (1, z + s < nz)]

    for s in range(1, nz):
        for way, there in ways(s):
            b = ((z - s + nz) % nz if way == 0 else (z + s) % nz) * ny + y

            @pl.when(there)
            def _():
                for c in range(cuts):
                    arrive(b, c).wait_recv()
                    if s < nz - 1:
                        if way == 0:
                            @pl.when(z < nz - 1)
                            def _():
                                up(s, b, c).start()
                        else:
                            @pl.when(z > 0)
                            def _():
                                down(s, b, c).start()
                    for d in range(1, ny):
                        side(s, b, c, d, way).start()
                product(s, b)

            hand_on()
            pending.append((there, b))

        for way, there in ways(s - 1):
            from_side(s - 1, way, there)

    for way, there in ways(nz - 1):
        from_side(nz - 1, way, there)
    hand_on()

    for slot in range(per):
        acc = total[slot]
        for d in range(1, tp):
            at = (d - 1) * per + slot
            remote(landed.at[at], landed.at[at], part_sem.at[0], land_sem.at[at], me, mine).wait_recv()
            acc = acc + landed[at].astype(F32)
        out_ref[slot * rows : (slot + 1) * rows] = acc.astype(BF16)

    for s in range(nz):
        for way, there in ways(s):
            b = ((z - s + nz) % nz if way == 0 else (z + s) % nz) * ny + y

            @pl.when(there)
            def _():
                for c in range(cuts):
                    if s < nz - 1:
                        if way == 0:
                            @pl.when(z < nz - 1)
                            def _():
                                up(s, b, c).wait_send()
                        if way == 1 or s == 0:
                            @pl.when(z > 0)
                            def _():
                                down(s, b, c).wait_send()
                    for d in range(1, ny):
                        side(s, b, c, d, way).wait_send()
    for b in range(kv):
        @pl.when(b // per != mine)
        def _():
            hand(b).wait_send()


def spread_out(hidden, weight, ny, nz, tp):
    rows, width = hidden.shape
    cols = weight.shape[1]
    kv = ny * nz
    per = kv // tp
    cuts = 4
    vmem = pl.BlockSpec(memory_space=pltpu.VMEM)
    dma = pltpu.SemaphoreType.DMA
    return pl.pallas_call(
        functools.partial(spread_kernel, ny, nz, tp, cuts),
        out_shape=jax.ShapeDtypeStruct((per * rows, cols), BF16),
        in_specs=[vmem, vmem],
        out_specs=vmem,
        scratch_shapes=[
            pltpu.VMEM((kv, rows, width), BF16),
            pltpu.VMEM((kv, rows, cols), BF16),
            pltpu.VMEM(((tp - 1) * per, rows, cols), BF16),
            pltpu.VMEM((per, rows, cols), F32),
            dma((nz, cuts)),
            dma((nz, cuts)),
            dma((2, nz, max(ny - 1, 1), cuts)),
            dma((kv, cuts)),
            dma((kv,)),
            dma(((tp - 1) * per,)),
        ],
        compiler_params=pltpu.CompilerParams(
            collective_id=0, has_side_effects=True, vmem_limit_bytes=16 << 20
        ),
        cost_estimate=pl.CostEstimate(
            flops=2 * kv * rows * width * cols, bytes_accessed=8 * rows * width, transcendentals=0
        ),
        name="spread",
    )(hidden, weight)


def gather_sums_kernel(
    ny, nz, lag, tok_hbm, gain_ref, gate_ref, q_hbm, k_hbm, v_hbm, o_hbm, state_hbm,
    pk_ref, pv_ref, pin_ref, pfo_ref, stable_ref, count_ref, normal_ref,
    q_out, rest_out, gates_out, state_out, mat, normal_out, stable_out,
    tok, normed, wq, wrest, flat,
    side_out, side_in, line_out, below, above, last_out, last_in,
    flat_out, flat_below, flat_above, flat_last_out, flat_last_in,
    wide, kt, vw, decay, work,
    load_sem, side_sem, side_got, line_sem, below_got, above_got, last_sem, last_got,
    fline_sem, fbelow_got, fabove_got, flast_sem, flast_got, state_sem,
):
    me = lax.axis_index("kv")
    mine = lax.axis_index("tp")
    z, y = me // ny, lax.rem(me, ny)
    rows = q_out.shape[0]
    width = wq.shape[1]
    chunks = wrest.shape[0]
    units = ny + chunks
    seqs, heads = mat.shape[:2]
    depth = tok.shape[1]

    loads = [
        pltpu.make_async_copy(tok_hbm, tok, load_sem.at[0]),
        pltpu.make_async_copy(q_hbm, wq, load_sem.at[1]),
    ]
    for n, (w, at) in enumerate(
        [(w, at) for w in (k_hbm, v_hbm, o_hbm) for at in range(0, w.shape[1], width)]
    ):
        loads.append(
            pltpu.make_async_copy(w.at[:, pl.ds(at, width)], wrest.at[n], load_sem.at[2 + n])
        )
    for load in loads:
        load.start()

    def state_load(s):
        return pltpu.make_async_copy(state_hbm.at[s], mat.at[s], state_sem.at[s])

    greet(
        [((z + d) % nz * ny + y, mine) for d in sorted({1 % nz, nz - 1}) if d]
        + [(z * ny + (y + d) % ny, mine) for d in range(1, ny)]
    )
    loads[0].wait()
    gain = gain_ref[:, pl.ds(pl.multiple_of(me * depth, LANES), depth)]

    def prepare(n, carry):
        at = pl.ds(pl.multiple_of(n * rows, rows), rows)
        normed[at, :] = (tok[at, :].astype(F32) * gain).astype(BF16)
        return carry

    lax.fori_loop(0, ny * nz, prepare, 0)
    for load in loads[1:]:
        load.wait()

    small = flat.shape[1] - 8
    row = lax.broadcasted_iota(jnp.int32, (small, 2 * HEADS), 0)
    col = lax.broadcasted_iota(jnp.int32, (small, 2 * HEADS), 1)
    want = jnp.where(row < heads, row, HEADS - heads + row) + mine * heads
    picked = jnp.where(jnp.logical_and(row < 2 * heads, col == want), 1.0, 0.0).astype(BF16)
    gate_rows = jnp.dot(picked, gate_ref[...], preferred_element_type=F32).astype(BF16)

    def flats(n, carry):
        at = pl.ds(pl.multiple_of(n * rows, rows), rows)
        x = tok[at, :].astype(F32)
        full = x * x
        lead = full.astype(BF16)
        rest = (full - lead.astype(F32)).astype(BF16)
        ones = jnp.ones((8, depth), BF16)

        def across(a, b):
            return lax.dot_general(a, b, (((1,), (1,)), ((), ())), preferred_element_type=F32)

        flat[n] = jnp.concatenate(
            [across(gate_rows, normed[at, :]), across(ones, lead) + across(ones, rest)], axis=0
        )
        return carry

    def term(block, w):
        at = pl.ds(pl.multiple_of(block * rows, rows), rows)
        return jnp.dot(normed[at, :], w, preferred_element_type=F32)

    def side(d, p, j):
        u = p * chunks + j
        return remote(
            side_out.at[d - 1, u], side_in.at[ny - d - 1, u], side_sem.at[d - 1, u],
            side_got.at[ny - d - 1, u], z * ny + (y + d) % ny, mine,
        )

    def line(going_up, slot):
        got, sem, far = (below, below_got, me + ny) if going_up else (above, above_got, me - ny)
        return remote(line_out.at[slot], got.at[slot], line_sem.at[slot], sem.at[slot], far, mine)

    def flat_line(going_up, b):
        got, sem, far = (
            (flat_below, fbelow_got, me + ny) if going_up else (flat_above, fabove_got, me - ny)
        )
        return remote(flat_out.at[b], got.at[b], fline_sem.at[b], sem.at[b], far, mine)

    def last(d):
        return remote(
            last_out.at[d - 1], last_in.at[ny - d - 1], last_sem.at[d - 1],
            last_got.at[ny - d - 1], z * ny + (y + d) % ny, mine,
        )

    def flat_last(d):
        return remote(
            flat_last_out.at[d - 1], flat_last_in.at[ny - d - 1], flast_sem.at[d - 1],
            flast_got.at[ny - d - 1], z * ny + (y + d) % ny, mine,
        )

    def arrived(ref, sem):
        remote(ref, ref, load_sem.at[0], sem, me, mine).wait_recv()

    def fill_side(p, j):
        for d in range(1, ny):
            work[...] = term(p * ny + (y + d) % ny, wrest[j])

            def put(fine):
                side_out[d - 1, p * chunks + j] = fold(work[...], fine)

            by_kind(j, put)

    def start_side(p, j):
        for d in range(1, ny):
            side(d, p, j).start()

    def each_side(n, act):
        i, j = n // chunks, n % chunks

        @pl.when(jnp.logical_and(i < nz - 1, nz - 1 - i > z))
        def _():
            act(nz - 1 - i, j)

        @pl.when(i < z)
        def _():
            act(i, j)

        @pl.when(i == nz - 1)
        def _():
            act(z, j)

    def side_round(n, carry):
        each_side(n, fill_side)

        @pl.when(n > 0)
        def _():
            each_side(n - 1, start_side)

        return carry

    def add(ref, at, sem, j):
        arrived(ref.at[at], sem.at[at])

        def more(fine):
            work[...] = work[...] + unfold(ref[at], fine)

        by_kind(j, more)

    def add_sides(p, j):
        for d in range(1, ny):
            add(side_in, (d - 1, p * chunks + j), side_got, j)

    def pass_on(going_up, slot, j):
        got, sem = (below, below_got) if going_up else (above, above_got)

        @pl.when(z > 0 if going_up else z < nz - 1)
        def _():
            add(got, slot, sem, j)

        def put(fine):
            line_out[slot] = fold(work[...], fine)

        by_kind(j, put)

    def pass_flat(going_up, b):
        got, sem = (flat_below, fbelow_got) if going_up else (flat_above, fabove_got)
        first = z == 0 if going_up else z == nz - 1

        @pl.when(first)
        def _():
            flat_out[b] = flat[b]

        @pl.when(jnp.logical_not(first))
        def _():
            arrived(got.at[b], sem.at[b])
            flat_out[b] = flat[b] + got[b]

    early = (nz - 1) * ny
    total = early + (nz - 1) * chunks

    def plane_of(going_up, i):
        return nz - 1 - i if going_up else i

    def flow(going_up, n, send):
        @pl.when(jnp.logical_and(n >= 0, n < early))
        def _():
            p = plane_of(going_up, n // ny)

            @pl.when(p > z if going_up else p < z)
            def _():
                b = p * ny + n % ny
                if send:
                    flat_line(going_up, b).start()
                    line(going_up, p * units + n % ny).start()
                else:
                    pass_flat(going_up, b)
                    work[...] = term(b, wq[...])
                    pass_on(going_up, p * units + n % ny, 0)

        @pl.when(jnp.logical_and(n >= early, n < total))
        def _():
            p = plane_of(going_up, (n - early) // chunks)
            j = (n - early) % chunks

            @pl.when(p > z if going_up else p < z)
            def _():
                slot = p * units + ny + j
                if send:
                    line(going_up, slot).start()
                else:
                    work[...] = term(p * ny + y, wrest[j])
                    add_sides(p, j)
                    pass_on(going_up, slot, j)

    def close_query():
        for d in range(ny):
            yy = (y + d) % ny
            b, slot = z * ny + yy, z * units + yy
            acc = term(b, wq[...])
            small = flat[b]

            def keep(acc, small):
                if d == 0:
                    q_out[...] = acc
                    flat_out[b] = small
                else:
                    last_out[d - 1] = fold(acc, True)
                    flat_last_out[d - 1] = small

            def lower():
                arrived(below.at[slot], below_got.at[slot])
                arrived(flat_below.at[b], fbelow_got.at[b])
                return unfold(below[slot], True), flat_below[b]

            def upper():
                arrived(above.at[slot], above_got.at[slot])
                arrived(flat_above.at[b], fabove_got.at[b])
                return unfold(above[slot], True), flat_above[b]

            @pl.when(z == 0)
            def _():
                more, less = upper()
                keep(acc + more, small + less)

            @pl.when(z == nz - 1)
            def _():
                more, less = lower()
                keep(acc + more, small + less)

            @pl.when(jnp.logical_and(z > 0, z < nz - 1))
            def _():
                more, less = lower()
                again, still = upper()
                keep(acc + more + again, small + less + still)


    def exact(a, b):
        return jnp.dot(a, b, precision=HP, preferred_element_type=F32)

    def prepare_commit():
        run = None
        sums, lives = [], []
        for p in range(PROP):
            live = count_ref[...] > p
            here = jnp.where(live, pfo_ref[p], 0.0)
            run = here if run is None else run + here
            sums.append(run)
            lives.append(live)
        logs = [
            jnp.where(live, run - part + pin_ref[p], NEG)
            for p, (live, part) in enumerate(zip(lives, sums))
        ]
        carried = run + stable_ref[...]
        top = carried
        for log in logs:
            top = jnp.maximum(top, log)
        stable_out[...] = top
        seq = lax.broadcasted_iota(jnp.int32, (seqs, rows), 0)
        at = lax.broadcasted_iota(jnp.int32, (seqs, rows), 1)
        flat_weights = None
        for p, log in enumerate(logs):
            got = exact(jnp.exp(log - top), (at == seq * PROP + p).astype(F32))
            flat_weights = got if flat_weights is None else flat_weights + got
        spare = jnp.zeros((LANES - heads, rows), F32)
        weights = jnp.concatenate([flat_weights, spare], axis=0).T
        lanes = (
            lax.broadcasted_iota(jnp.int32, (seqs, LANES), 0)
            == lax.broadcasted_iota(jnp.int32, (seqs, LANES), 1)
        ).astype(F32)
        flat_decay = jnp.concatenate(
            [exact(jnp.exp(carried - top), lanes), jnp.zeros((LANES - heads, LANES), F32)], axis=0
        ).T

        pair = 8 // PROP

        def gather_keys(i, carry):
            to = pl.ds(pl.multiple_of(i * 8, 8), 8)
            got = [pk_ref[i * pair + n].astype(F32) for n in range(pair)]
            wide[to, : heads * DQK] = jnp.concatenate(got, axis=0)
            return carry

        lax.fori_loop(0, seqs // pair, gather_keys, 0)
        for h in range(heads):
            keys = wide[:, h * DQK : (h + 1) * DQK]
            kt[h] = keys.T
            mine_only = jnp.where(at // PROP == seq, flat_weights[h : h + 1], 0.0)
            fade = jnp.broadcast_to(flat_decay[:seqs, h : h + 1], (seqs, DV))
            decay[h] = fade
            normal_out[h] = fade[:, :DQK] * normal_ref[:, h, :] + exact(mine_only, keys)

        def gather_values(i, carry):
            to = pl.ds(pl.multiple_of(i * 8, 8), 8)
            got = [pv_ref[i * pair + n].astype(F32) for n in range(pair)]
            wide[to, :] = jnp.concatenate(got, axis=0)
            return carry

        lax.fori_loop(0, seqs // pair, gather_values, 0)
        for h in range(heads):
            at_h = slice(h * DV, (h + 1) * DV)
            lead, rest = two_terms(wide[:, at_h] * weights[:, h : h + 1])
            vw[:rows, at_h] = lead
            vw[rows:, at_h] = rest

    def commit(s):
        state_load(s).wait()
        own = lax.broadcasted_iota(jnp.int32, (DQK, rows), 1) // PROP == s
        for h in range(heads):
            lhs = jnp.where(own, kt[h], 0.0).astype(BF16)
            lhs = jnp.concatenate([lhs, lhs], axis=1)
            added = jnp.dot(lhs, vw[:, h * DV : (h + 1) * DV], preferred_element_type=F32)
            mat[s, h] = decay[h, pl.ds(s, 1), :] * mat[s, h] + added

    def finish_query():
        for d in range(1, ny):
            arrived(last_in.at[d - 1], last_got.at[d - 1])
            q_out[...] = q_out[...] + unfold(last_in[d - 1], True)

    def state_product(g):
        at = pl.ds(pl.multiple_of(g * 16, 16), 16)
        row16 = lax.broadcasted_iota(jnp.int32, (16, 1), 0) // PROP
        for h in range(heads):
            part, less = two_terms(q_out[at, h * DQK : (h + 1) * DQK])
            both = jnp.concatenate([part, less], axis=0)
            got = None
            for n in range(16 // PROP):
                lead, rest = two_terms(mat[g * (16 // PROP) + n, h])
                res = jnp.dot(both, lead, preferred_element_type=F32)
                res = res[:16] + res[16:] + jnp.dot(part, rest, preferred_element_type=F32)
                got = res if got is None else jnp.where(row16 == n, res, got)
            state_out[at, h * DV : (h + 1) * DV] = got

    lax.fori_loop(0, chunks + 1, side_round, 0)
    lax.fori_loop(0, ny * nz, flats, 0)
    close_at = early + lag * (nz - 1) + 1
    groups = rows // 16
    product_at = max(close_at + 2, 2 + seqs // 2)

    def step(n, carry):
        up_at, down_at = n - lag * z, n - lag * (nz - 1 - z)
        flow(True, up_at, False)
        flow(False, down_at, False)
        flow(True, up_at, True)
        flow(False, down_at, True)

        @pl.when(n == close_at)
        def _():
            close_query()

        @pl.when(jnp.logical_and(n >= 2, n < 2 + seqs // 2))
        def _():
            commit(2 * (n - 2))

        @pl.when(n == product_at)
        def _():
            finish_query()

        @pl.when(n == close_at)
        def _():
            for d in range(1, ny):
                last(d).start()
                flat_last(d).start()

        @pl.when(n == 1)
        def _():
            lax.fori_loop(chunks + 1, nz * chunks, side_round, 0)
            each_side(nz * chunks - 1, start_side)
            for s in range(seqs):
                state_load(s).start()
            prepare_commit()

        @pl.when(jnp.logical_and(n >= 2, n < 2 + seqs // 2))
        def _():
            commit(2 * (n - 2) + 1)

        @pl.when(jnp.logical_and(n >= product_at, n < product_at + groups))
        def _():
            state_product(n - product_at)

        return carry

    lax.fori_loop(0, max(total + lag * (nz - 1), product_at + groups), step, 0)

    def close_rest(j, carry):
        slot = z * units + ny + j
        work[...] = term(me, wrest[j])
        add_sides(z, j)

        @pl.when(z > 0)
        def _():
            add(below, slot, below_got, j)

        @pl.when(z < nz - 1)
        def _():
            add(above, slot, above_got, j)

        at = pl.ds(pl.multiple_of(j * width, width), width)
        rest_out[:, at] = work[...]
        return carry

    lax.fori_loop(0, chunks, close_rest, 0)
    small = flat_out[me]
    for d in range(1, ny):
        arrived(flat_last_in.at[d - 1], flast_got.at[d - 1])
        small = small + flat_last_in[d - 1]
    spare = jnp.zeros((LANES - small.shape[0], rows), F32)
    gates_out[...] = jnp.concatenate([small, spare], axis=0).T

    for d in range(1, ny):
        last(d).wait_send()
        flat_last(d).wait_send()

    def drain_side(u, carry):
        for d in range(1, ny):
            side(d, u // chunks, u % chunks).wait_send()
        return carry

    lax.fori_loop(0, nz * chunks, drain_side, 0)

    def drain_line(slot, carry):
        p = slot // units

        @pl.when(p > z)
        def _():
            line(True, slot).wait_send()

        @pl.when(p < z)
        def _():
            line(False, slot).wait_send()

        return carry

    lax.fori_loop(0, nz * units, drain_line, 0)

    def drain_flat(b, carry):
        @pl.when(b // ny > z)
        def _():
            flat_line(True, b).wait_send()

        @pl.when(b // ny < z)
        def _():
            flat_line(False, b).wait_send()

        return carry

    lax.fori_loop(0, nz * ny, drain_flat, 0)


def gather_sums(
    tokens, gain, gates, query, key, value, outgate, state, prior_keys, prior_values,
    ingate, forget, stable, count, normal, ny, nz,
):
    kv = ny * nz
    depth = tokens.shape[1]
    rows = tokens.shape[0] // kv
    width = query.shape[1]
    chunks = (key.shape[1] + value.shape[1] + outgate.shape[1]) // width
    units = ny + chunks
    seqs, heads = state.shape[:2]
    small = -(-2 * heads // 8) * 8 + 8
    others = max(ny - 1, 1)
    vmem = pl.BlockSpec(memory_space=pltpu.VMEM)
    anywhere = pl.BlockSpec(memory_space=pl.ANY)
    dma = pltpu.SemaphoreType.DMA
    unit = (rows, width)
    tiny = (small, rows)
    return pl.pallas_call(
        functools.partial(gather_sums_kernel, ny, nz, 2),
        out_shape=[
            pltpu.VMEM(unit, F32),
            pltpu.VMEM((rows, chunks * width), F32),
            pltpu.VMEM((rows, LANES), F32),
            pltpu.VMEM((rows, heads * DV), F32),
            pltpu.VMEM(state.shape, F32),
            pltpu.VMEM((heads, seqs, DQK), F32),
            pltpu.VMEM((heads, seqs), F32),
        ],
        in_specs=[anywhere, vmem, vmem] + [anywhere] * 5 + [vmem] * 7,
        out_specs=[vmem] * 7,
        scratch_shapes=[
            pltpu.VMEM(tokens.shape, BF16),
            pltpu.VMEM(tokens.shape, BF16),
            pltpu.VMEM((depth, width), BF16),
            pltpu.VMEM((chunks, depth, width), BF16),
            pltpu.VMEM((kv,) + tiny, F32),
            pltpu.VMEM((others, nz * chunks) + unit, BF16),
            pltpu.VMEM((others, nz * chunks) + unit, BF16),
            pltpu.VMEM((nz * units,) + unit, BF16),
            pltpu.VMEM((nz * units,) + unit, BF16),
            pltpu.VMEM((nz * units,) + unit, BF16),
            pltpu.VMEM((others,) + unit, BF16),
            pltpu.VMEM((others,) + unit, BF16),
            pltpu.VMEM((kv,) + tiny, F32),
            pltpu.VMEM((kv,) + tiny, F32),
            pltpu.VMEM((kv,) + tiny, F32),
            pltpu.VMEM((others,) + tiny, F32),
            pltpu.VMEM((others,) + tiny, F32),
            pltpu.VMEM((rows, heads * DV), F32),
            pltpu.VMEM((heads, DQK, rows), F32),
            pltpu.VMEM((2 * rows, heads * DV), BF16),
            pltpu.VMEM((heads, seqs, DV), F32),
            pltpu.VMEM(unit, F32),
            dma((2 + chunks,)),
            dma((others, nz * chunks)),
            dma((others, nz * chunks)),
            dma((nz * units,)),
            dma((nz * units,)),
            dma((nz * units,)),
            dma((others,)),
            dma((others,)),
            dma((kv,)),
            dma((kv,)),
            dma((kv,)),
            dma((others,)),
            dma((others,)),
            dma((seqs,)),
        ],
        compiler_params=pltpu.CompilerParams(
            collective_id=1, has_side_effects=True, vmem_limit_bytes=36 << 20
        ),
        cost_estimate=pl.CostEstimate(
            flops=2 * kv * rows * depth * width * (chunks + 1),
            bytes_accessed=2 * depth * width * (chunks + 1) + 4 * state.size,
            transcendentals=0,
        ),
        name="gather_sums",
    )(
        tokens, gain, gates, query, key, value, outgate, state, prior_keys, prior_values,
        ingate, forget, stable, count, normal,
    )


def per_device(
    kv,
    tp,
    tokens,
    norm_gain,
    query_weight,
    key_weight,
    value_weight,
    outgate_weight,
    gate_weight,
    forget_bias,
    head_gain,
    output_weight,
    state_matrix,
    state_normal,
    state_stable,
    prior_keys,
    prior_values,
    prior_ingate,
    prior_forget,
    accepted,
    parents,
):
    ny = 1 << ((kv.bit_length() - 1) // 2)
    nz = kv // ny
    query, rest, gates, state, matrix, normal, stable = gather_sums(
        tokens,
        norm_gain[None, :],
        gate_weight.T,
        query_weight,
        key_weight,
        value_weight,
        outgate_weight,
        state_matrix,
        prior_keys,
        prior_values,
        prior_ingate.transpose(1, 2, 0),
        prior_forget.transpose(1, 2, 0),
        state_stable.T,
        accepted[None, :],
        state_normal,
        ny,
        nz,
    )
    hidden, new_matrix, new_normal, new_stable = tree_read(
        query,
        rest,
        gates,
        state,
        matrix,
        normal,
        stable,
        parents.T,
        forget_bias[None, :],
        head_gain[None, :],
    )
    layer_out = spread_out(hidden, output_weight, ny, nz, tp)
    return (layer_out, new_matrix, new_normal, new_stable.T)


def solution(mesh):
    placed = (
        P(None, "kv"),
        P(),
        P("kv", "tp"),
        P("kv", "tp"),
        P("kv", "tp"),
        P("kv", "tp"),
        P("kv", None),
        P(),
        P("tp"),
        P("tp", "kv"),
        P("kv", "tp", None, None),
        P("kv", "tp", None),
        P("kv", "tp"),
        P("kv", None, "tp"),
        P("kv", None, "tp"),
        P("kv", None, "tp"),
        P("kv", None, "tp"),
        P("kv"),
        P("kv", None),
    )
    return jax.shard_map(
        functools.partial(per_device, mesh.shape["kv"], mesh.shape["tp"]),
        mesh=mesh,
        in_specs=placed,
        out_specs=(P("tp", "kv"), P("kv", "tp", None, None), P("kv", "tp", None), P("kv", "tp")),
        check_vma=False,
    )
```
